128 devices in a mesh: fs: 16 (over z, y), tp: 8 (over x, core).
Axes of the slice: x: 4, y: 4, z: 4, core: 2. Of those that a mesh axis runs over, the one named last changes fastest.
Arguments:
- inputs: bfloat16 [49152, 2048], P('fs'), may hold values from -6 to 6
- cot_query: bfloat16 [49152, 2048], P('fs', 'tp'), may hold values from -0.0625 to 0.0625
- cot_value: bfloat16 [49152, 4096], P('fs', 'tp'), may hold values from -0.0625 to 0.0625
- proj_query: bfloat16 [2048, 256], replicated, may hold values from -0.375 to 0.375
- proj_value: bfloat16 [2048, 256], replicated, may hold values from -0.375 to 0.375
- w_query: float32 [2048, 2048], P('fs', 'tp'), may hold values from -6 to 6
- w_value: float32 [2048, 4096], P('fs', 'tp'), may hold values from -6 to 6
- m_query: float32 [256, 2048], P('fs', 'tp'), may hold values from -30 to 30
- m_value: float32 [256, 4096], P('fs', 'tp'), may hold values from -30 to 30
- v_query: float32 [256, 2048], P('fs', 'tp'), may hold values from 0.05 to 2
- v_value: float32 [256, 4096], P('fs', 'tp'), may hold values from 0.05 to 2
Outputs:
- new_query: float32 [2048, 2048], P('fs', 'tp')
- new_value: float32 [2048, 4096], P('fs', 'tp')
- copy_query: bfloat16 [2048, 2048], P(None, 'tp')
- copy_value: bfloat16 [2048, 4096], P(None, 'tp')
- first_query: float32 [256, 2048], P('fs', 'tp')
- first_value: float32 [256, 4096], P('fs', 'tp')
- second_query: float32 [256, 2048], P('fs', 'tp')
- second_value: float32 [256, 4096], P('fs', 'tp')
- step_query: float32 [2048, 2048], P('fs', 'tp')
- step_value: float32 [2048, 4096], P('fs', 'tp')
The draws below stay inside these ranges and needn't reach their ends.
All inputs are finite; a program needn't handle non-finite values.
Results may differ from the reference program's by a relative error of at most 0.015.
Values may be sent and summed in bfloat16 or wider, within the bound.
No kernel may reach another device: no remote copies, remote signals or barrier semaphores. Data moves between devices by JAX's collectives and lax.ppermute only.
A program may use at most 128 MiB of HBM per device.

```python
import math
import jax
import jax.numpy as jnp
from jax import lax

D = 2048
RANK = 256
QK_W = 2048
V_W = 4096
TOKENS = 49152


def moment_draw(key, rows, cols):
    base = jax.random.normal(jax.random.fold_in(key, 11), (rows, cols), jnp.float32)
    base = jnp.clip(base, -5.0, 5.0) * 0.5
    row_scale = (4.0 ** (jnp.arange(rows, dtype=jnp.float32) / rows))[:, None]
    col_scale = (3.0 ** (jnp.arange(cols, dtype=jnp.float32) / cols))[None, :]
    return base * row_scale * col_scale


def draw_m_query(key, part):
    return moment_draw(key, RANK, QK_W)


def draw_m_value(key, part):
    return moment_draw(key, RANK, V_W)


def levels(stream_key, shape, pieces, low, high):
    def one(axis_at, parts):
        draws = jax.random.uniform(jax.random.fold_in(jax.random.fold_in(stream_key, 6), axis_at), (parts,), jnp.float32, low / len(pieces), high / len(pieces))
        return jnp.repeat(jnp.exp(draws), shape[axis_at] // parts).reshape((-1,) + (1,) * (len(shape) - axis_at - 1))

    loudness = one(*pieces[0])
    for cut in pieces[1:]:
        loudness = loudness * one(*cut)
    return loudness


def normal_values(own_key, extent, scale, limit, cuts=(), held_as=jnp.bfloat16):
    loudness = levels(own_key, extent, cuts, -0.22, 0.18) if cuts else 1.0
    drawn = jax.random.normal(own_key, extent, jnp.float32) * scale * loudness
    return jnp.minimum(jnp.maximum(drawn, -limit), limit).astype(held_as)


def setup_inputs(seed: int = 0) -> dict:
    splits = jax.random.split(jax.random.key(seed), 12)
    return {
        "inputs": normal_values(splits[0], (TOKENS, D), 1.0, 6.0, ((0, 16),)),
        "cot_query": normal_values(splits[1], (TOKENS, QK_W), (TOKENS ** -0.5), 0.0625, ((0, 16), (1, 8))),
        "cot_value": normal_values(splits[2], (TOKENS, V_W), (TOKENS ** -0.5), 0.0625, ((0, 16), (1, 8))),
        "proj_query": normal_values(splits[3], (D, RANK), RANK ** -0.5, 0.375),
        "proj_value": normal_values(splits[4], (D, RANK), RANK ** -0.5, 0.375),
        "w_query": normal_values(splits[5], (D, QK_W), 1.0, 6.0, ((0, 16), (1, 8)), jnp.float32),
        "w_value": normal_values(splits[6], (D, V_W), 1.0, 6.0, ((0, 16), (1, 8)), jnp.float32),
        "m_query": draw_m_query(jax.random.fold_in(splits[11], 71), 0),
        "m_value": draw_m_value(jax.random.fold_in(splits[11], 71), 0),
        "v_query": jnp.clip(jnp.exp(math.log(2.0) - 3.6888794 * jax.random.uniform(splits[9], (RANK, QK_W), jnp.float32) ** levels(splits[9], (RANK, QK_W), ((0, 16), (1, 8)), -0.2, 0.2)), 0.05, 2.0),
        "v_value": jnp.clip(jnp.exp(math.log(2.0) - 3.6888794 * jax.random.uniform(splits[10], (RANK, V_W), jnp.float32) ** levels(splits[10], (RANK, V_W), ((0, 16), (1, 8)), -0.2, 0.2)), 0.05, 2.0),
    }


beta_first = 0.9
beta_second = 0.95
adam_eps = 1e-08
norm_eps = 1e-06
step_rate = 0.05
decay_rate = 0.2

def moment_update(factor, gradient, first, second):
    low = jnp.dot(factor.astype(jnp.float32).T, gradient, precision=lax.Precision.HIGHEST)
    first_new = beta_first * first + (1.0 - beta_first) * low
    second_new = beta_second * second + (1.0 - beta_second) * low * low
    update = first_new / (jnp.sqrt(second_new) + adam_eps)
    return (first_new, second_new, update)

def reference(inputs, cot_query, cot_value, proj_query, proj_value, w_query, w_value, m_query, m_value, v_query, v_value):
    grad_query = jnp.dot(inputs.T, cot_query, preferred_element_type=jnp.float32)
    grad_value = jnp.dot(inputs.T, cot_value, preferred_element_type=jnp.float32)
    first_query, second_query, update_query = moment_update(proj_query, grad_query, m_query, v_query)
    first_value, second_value, update_value = moment_update(proj_value, grad_value, m_value, v_value)
    total = jnp.sum(update_query * update_query) + jnp.sum(update_value * update_value)
    scale = lax.rsqrt(total / (RANK * (QK_W + V_W)) + norm_eps)
    step_query = scale * jnp.dot(proj_query.astype(jnp.float32), update_query, precision=lax.Precision.HIGHEST) + decay_rate * w_query
    step_value = scale * jnp.dot(proj_value.astype(jnp.float32), update_value, precision=lax.Precision.HIGHEST) + decay_rate * w_value
    new_query = w_query - step_rate * step_query
    new_value = w_value - step_rate * step_value
    return (new_query, new_value, new_query.astype(jnp.bfloat16), new_value.astype(jnp.bfloat16), first_query, first_value, second_query, second_value, step_query, step_value)
```

```python
import jax
import jax.numpy as jnp
from jax import lax
from jax.experimental import pallas as pl
from jax.experimental.pallas import tpu as pltpu
from jax.sharding import Mesh
from jax.sharding import PartitionSpec as P

RANK = 256
QK_W = 2048
V_W = 4096
AXES = ("z", "y", "x", "c")
SIZES = (4, 4, 4, 2)
FS = ("z", "y")
TP = ("x", "c")

beta_first = 0.9
beta_second = 0.95
adam_eps = 1e-08
norm_eps = 1e-06
step_rate = 0.05
decay_rate = 0.2

WQ = 256
WV = 512
W = WQ + WV
ROWS = 128
TOKEN_BLOCK = 512

F32 = jnp.float32
BF16 = jnp.bfloat16


def shift_pairs(kind, offset):
    pairs = []
    for z in range(4):
        for y in range(4):
            for x in range(4):
                for c in range(2):
                    to = [z, y, x, c]
                    if kind == "major":
                        axis = 0 if c == 0 else 1
                    elif kind == "minor":
                        axis = 1 if c == 0 else 0
                    elif kind == "x":
                        axis = 2
                    else:
                        axis = 3
                    to[axis] = (to[axis] + offset) % SIZES[axis]
                    source = ((z * 4 + y) * 4 + x) * 2 + c
                    target = ((to[0] * 4 + to[1]) * 4 + to[2]) * 2 + to[3]
                    pairs.append((source, target))
    return pairs


def shifted(array, kind, offset):
    return lax.ppermute(array, AXES, shift_pairs(kind, offset))


def own_place():
    z, y, c = lax.axis_index("z"), lax.axis_index("y"), lax.axis_index("c")
    first = c == 0
    major = jnp.where(first, z, y)
    minor = jnp.where(first, y, z)
    per_major = jnp.where(first, 4, 1)
    per_minor = jnp.where(first, 1, 4)
    return major, minor, per_major, per_minor


def gradient_kernel(x, cq, cv, pq, pv, wq, wv, own, to_1, to_2, to_3, w16, total):
    step = pl.program_id(0)

    @pl.when(step == 0)
    def _():
        total[...] = jnp.zeros_like(total)
        w16[:, :WQ] = wq[...].astype(BF16)
        w16[:, WQ:] = wv[...].astype(BF16)

    rows = x[...]
    mixed_q = jnp.dot(rows, pq[...], preferred_element_type=F32).astype(BF16)
    mixed_v = jnp.dot(rows, pv[...], preferred_element_type=F32).astype(BF16)
    lead = (((0,), (0,)), ((), ()))
    total[:, :WQ] += lax.dot_general(mixed_q, cq[...], lead, preferred_element_type=F32)
    total[:, WQ:] += lax.dot_general(mixed_v, cv[...], lead, preferred_element_type=F32)

    @pl.when(step == pl.num_programs(0) - 1)
    def _():
        major, _, per_major, per_minor = own_place()
        for offset, out in enumerate((own, to_1, to_2, to_3)):
            there = lax.rem(major + offset, 4)
            for minor in range(4):
                start = pl.multiple_of((there * per_major + minor * per_minor) * 16, 16)
                out[minor * 16 : (minor + 1) * 16, :] = total[pl.ds(start, 16), :].astype(out.dtype)


def projected_gradient(inputs, cq, cv, pq, pv, wq, wv):
    tokens, width = inputs.shape
    whole = lambda a: pl.BlockSpec(a.shape, lambda i: (0, 0))
    by_tokens = lambda a: pl.BlockSpec((TOKEN_BLOCK, a.shape[1]), lambda i: (i, 0))
    out = [
        jax.ShapeDtypeStruct((64, W), F32),
        jax.ShapeDtypeStruct((64, W), BF16),
        jax.ShapeDtypeStruct((64, W), BF16),
        jax.ShapeDtypeStruct((64, W), BF16),
        jax.ShapeDtypeStruct((ROWS, W), BF16),
    ]
    return pl.pallas_call(
        gradient_kernel,
        grid=(tokens // TOKEN_BLOCK,),
        in_specs=[by_tokens(inputs), by_tokens(cq), by_tokens(cv)]
        + [whole(a) for a in (pq, pv, wq, wv)],
        out_specs=[whole(a) for a in out],
        out_shape=out,
        scratch_shapes=[pltpu.VMEM((RANK, W), F32)],
        cost_estimate=pl.CostEstimate(
            flops=2 * tokens * RANK * (2 * width + W), bytes_accessed=20_000_000, transcendentals=0
        ),
        name="gradient",
    )(inputs, cq, cv, pq, pv, wq, wv)


def whole_call(body, out, operands, scratch=(), flops=1_000_000):
    vmem = pl.BlockSpec(memory_space=pltpu.VMEM)
    return pl.pallas_call(
        body,
        in_specs=[vmem] * len(operands),
        out_specs=[vmem] * len(out),
        out_shape=out,
        scratch_shapes=list(scratch),
        cost_estimate=pl.CostEstimate(flops=flops, bytes_accessed=1_000_000, transcendentals=0),
    )(*operands)


def partial_kernel(own, r1, r2, r3, mq, mv, vq, vv, out):
    out[:64, :] = (own[...] + r1[...].astype(F32) + (r2[...].astype(F32) + r3[...].astype(F32))).astype(BF16)
    out[64:80, :WQ] = mq[...].astype(BF16)
    out[64:80, WQ:] = mv[...].astype(BF16)
    out[80:96, :WQ] = vq[...].astype(BF16)
    out[80:96, WQ:] = vv[...].astype(BF16)


def moments(low, first, second):
    first_new = beta_first * first + (1.0 - beta_first) * low
    second_new = beta_second * second + (1.0 - beta_second) * low * low
    return first_new, second_new


def update_kernel(own, r1, r2, r3, mq, mv, vq, vv, u, fq, fv, sq, sv, low):
    low[...] = (own[:64, :].astype(F32) + r2[:64, :].astype(F32)) + (
        r1[:64, :].astype(F32) + r3[:64, :].astype(F32)
    )
    _, minor, _, _ = own_place()
    for offset, held in enumerate((own, r1, r2, r3)):
        there = lax.rem(minor + 4 - offset, 4)
        at = pl.ds(pl.multiple_of(there * 16, 16), 16)
        first, second = moments(low[at, :], held[64:80, :].astype(F32), held[80:96, :].astype(F32))
        u[at, :] = (first / (jnp.sqrt(second) + adam_eps)).astype(BF16)
    mine = low[pl.ds(pl.multiple_of(minor * 16, 16), 16), :]
    fq[...], sq[...] = moments(mine[:, :WQ], mq[...], vq[...])
    fv[...], sv[...] = moments(mine[:, WQ:], mv[...], vv[...])


def assemble_kernel(own, r1, r2, r3, u, squares):
    major, _, per_major, per_minor = own_place()
    for offset, held in enumerate((own, r1, r2, r3)):
        there = lax.rem(major + 4 - offset, 4)
        for minor in range(4):
            start = pl.multiple_of((there * per_major + minor * per_minor) * 16, 16)
            u[pl.ds(start, 16), :] = held[minor * 16 : (minor + 1) * 16, :]
    total = jnp.zeros((16, W), F32)
    for group in range(16):
        part = u[group * 16 : (group + 1) * 16, :].astype(F32)
        total += part * part
    total = total[:8, :] + total[8:, :]
    folded = total[:, :128]
    for lane in range(1, W // 128):
        folded += total[:, lane * 128 : (lane + 1) * 128]
    squares[...] = folded


def weight_kernel(
    s_own, s_other, u, pq, pv, g0, g1, g2, g3, wq, wv,
    nq, nv, tq, tv, cq, cv,
    pq_s, pv_s, w_s, cq_s, cv_s, p_sem, w_sem, c_sem,
):
    loads = [pltpu.make_async_copy(pq, pq_s, p_sem.at[0]), pltpu.make_async_copy(pv, pv_s, p_sem.at[1])]
    groups = [pltpu.make_async_copy(g, w_s.at[i], w_sem.at[i]) for i, g in enumerate((g0, g1, g2, g3))]
    for copy in loads + groups:
        copy.start()
    major, minor, per_major, per_minor = own_place()
    squares = jnp.sum(s_own[...] + s_other[...], axis=(0, 1), keepdims=True)
    scale = lax.rsqrt(squares / (RANK * (QK_W + V_W)) + norm_eps)
    uq, uv = u[:, :WQ], u[:, WQ:]
    for copy in loads:
        copy.wait()
    stores = []
    for i in range(4):
        groups[i].wait()
        b_there = lax.rem(minor + 4 - i, 4)
        for j in range(4):
            a_there = lax.rem(major + 4 - j, 4)
            block = a_there * per_major + b_there * per_minor
            at = pl.ds(pl.multiple_of(block * ROWS, ROWS), ROWS)
            back_q = scale * jnp.dot(pq_s[at, :], uq, preferred_element_type=F32)
            back_v = scale * jnp.dot(pv_s[at, :], uv, preferred_element_type=F32)
            held = w_s[i, j * ROWS : (j + 1) * ROWS, :].astype(F32)
            n = i * 4 + j
            keep = 1.0 - step_rate * decay_rate
            cq_s[n] = (keep * held[:, :WQ] - step_rate * back_q).astype(BF16)
            cv_s[n] = (keep * held[:, WQ:] - step_rate * back_v).astype(BF16)
            for part, (source, target) in enumerate(((cq_s, cq), (cv_s, cv))):
                copy = pltpu.make_async_copy(source.at[n], target.at[at, :], c_sem.at[n, part])
                copy.start()
                stores.append(copy)
            if n == 0:
                for back, w, t, new in ((back_q, wq, tq, nq), (back_v, wv, tv, nv)):
                    weight = w[...]
                    step = back + decay_rate * weight
                    t[...] = step
                    new[...] = weight - step_rate * step
    for copy in stores:
        copy.wait()


def new_weights(s_own, s_other, u, pq, pv, groups, wq, wv):
    vmem = pl.BlockSpec(memory_space=pltpu.VMEM)
    hbm = pl.BlockSpec(memory_space=pl.ANY)
    out = [
        jax.ShapeDtypeStruct((ROWS, WQ), F32),
        jax.ShapeDtypeStruct((ROWS, WV), F32),
        jax.ShapeDtypeStruct((ROWS, WQ), F32),
        jax.ShapeDtypeStruct((ROWS, WV), F32),
        jax.ShapeDtypeStruct((16 * ROWS, WQ), BF16),
        jax.ShapeDtypeStruct((16 * ROWS, WV), BF16),
    ]
    return pl.pallas_call(
        weight_kernel,
        in_specs=[vmem] * 3 + [hbm] * 6 + [vmem] * 2,
        out_specs=[vmem] * 4 + [hbm] * 2,
        out_shape=out,
        scratch_shapes=[
            pltpu.VMEM((16 * ROWS, RANK), BF16),
            pltpu.VMEM((16 * ROWS, RANK), BF16),
            pltpu.VMEM((4, 4 * ROWS, W), BF16),
            pltpu.VMEM((16, ROWS, WQ), BF16),
            pltpu.VMEM((16, ROWS, WV), BF16),
            pltpu.SemaphoreType.DMA((2,)),
            pltpu.SemaphoreType.DMA((4,)),
            pltpu.SemaphoreType.DMA((16, 2)),
        ],
        cost_estimate=pl.CostEstimate(
            flops=2 * 16 * ROWS * RANK * W, bytes_accessed=12_000_000, transcendentals=0
        ),
        name="weights",
    )(s_own, s_other, u, pq, pv, *groups, wq, wv)


def on_device(inputs, cq, cv, pq, pv, wq, wv, mq, mv, vq, vv):
    own, to_1, to_2, to_3, w16 = projected_gradient(inputs, cq, cv, pq, pv, wq, wv)
    parts = [shifted(a, "major", n) for n, a in ((2, to_2), (1, to_1), (3, to_3))]
    w_1, w_2, w_3 = (shifted(w16, "major", n) for n in (1, 2, 3))
    message, = whole_call(
        partial_kernel, [jax.ShapeDtypeStruct((96, W), BF16)], (own, *parts, mq, mv, vq, vv)
    )
    m_2, m_1, m_3 = (shifted(message, "minor", n) for n in (2, 1, 3))
    group = jnp.concatenate([w16, w_1, w_2, w_3], axis=0)
    g_1, g_2, g_3 = (shifted(group, "minor", n) for n in (1, 2, 3))
    small = lambda n: jax.ShapeDtypeStruct((16, n), F32)
    u_own, first_q, first_v, second_q, second_v = whole_call(
        update_kernel,
        [jax.ShapeDtypeStruct((64, W), BF16), small(WQ), small(WV), small(WQ), small(WV)],
        (message, m_1, m_2, m_3, mq, mv, vq, vv),
        [pltpu.VMEM((64, W), F32)],
    )
    u_2, u_1, u_3 = (shifted(u_own, "major", n) for n in (2, 1, 3))
    u, squares = whole_call(
        assemble_kernel,
        [jax.ShapeDtypeStruct((RANK, W), BF16), jax.ShapeDtypeStruct((8, 128), F32)],
        (u_own, u_1, u_2, u_3),
    )
    s_2, s_1, s_3 = (shifted(squares, "x", n) for n in (2, 1, 3))
    chips = (squares + s_2) + (s_1 + s_3)
    other = shifted(chips, "core", 1)
    new_q, new_v, step_q, step_v, copy_q, copy_v = new_weights(
        chips, other, u, pq, pv, (group, g_1, g_2, g_3), wq, wv
    )
    return (new_q, new_v, copy_q, copy_v, first_q, first_v, second_q, second_v, step_q, step_v)


def solution(mesh):
    finer = Mesh(mesh.devices.reshape(SIZES), AXES)
    both, tokens, columns = P(FS, TP), P(FS, None), P(None, TP)
    return jax.shard_map(
        on_device,
        mesh=finer,
        in_specs=(tokens, both, both, P(), P()) + (both,) * 6,
        out_specs=(both, both, columns, columns) + (both,) * 6,
        check_vma=False,
    )
```

```python
import jax
import jax.numpy as jnp
from jax import lax
from jax.experimental import pallas as pl
from jax.experimental.pallas import tpu as pltpu
from jax.sharding import Mesh
from jax.sharding import PartitionSpec as P

RANK = 256
QK_W = 2048
V_W = 4096
AXES = ("z", "y", "x", "c")
SIZES = (4, 4, 4, 2)
FS = ("z", "y")
TP = ("x", "c")

beta_first = 0.9
beta_second = 0.95
adam_eps = 1e-08
norm_eps = 1e-06
step_rate = 0.05
decay_rate = 0.2

WQ = 256
WV = 512
W = WQ + WV
ROWS = 128
TOKEN_BLOCK = 768

F32 = jnp.float32
BF16 = jnp.bfloat16


def shift_pairs(kind, offset):
    pairs = []
    for z in range(4):
        for y in range(4):
            for x in range(4):
                for c in range(2):
                    to = [z, y, x, c]
                    if kind == "major":
                        axis = 0 if c == 0 else 1
                    elif kind == "minor":
                        axis = 1 if c == 0 else 0
                    elif kind == "x":
                        axis = 2
                    else:
                        axis = 3
                    to[axis] = (to[axis] + offset) % SIZES[axis]
                    source = ((z * 4 + y) * 4 + x) * 2 + c
                    target = ((to[0] * 4 + to[1]) * 4 + to[2]) * 2 + to[3]
                    pairs.append((source, target))
    return pairs


def shifted(array, kind, offset):
    return lax.ppermute(array, AXES, shift_pairs(kind, offset))


def own_place():
    z, y, c = lax.axis_index("z"), lax.axis_index("y"), lax.axis_index("c")
    first = c == 0
    major = jnp.where(first, z, y)
    minor = jnp.where(first, y, z)
    per_major = jnp.where(first, 4, 1)
    per_minor = jnp.where(first, 1, 4)
    return major, minor, per_major, per_minor


def in_vmem(array):
    return pltpu.with_memory_space_constraint(array, pltpu.VMEM)


def gradient_kernel(x, cq, cv, pq, pv, wq, wv, own, to_1, to_2, to_3, w16, total):
    step = pl.program_id(0)

    @pl.when(step == 0)
    def _():
        total[...] = jnp.zeros_like(total)
        w16[:, :WQ] = wq[...].astype(BF16)
        w16[:, WQ:] = wv[...].astype(BF16)

    rows = x[...]
    mixed_q = jnp.dot(rows, pq[...], preferred_element_type=F32).astype(BF16)
    mixed_v = jnp.dot(rows, pv[...], preferred_element_type=F32).astype(BF16)
    lead = (((0,), (0,)), ((), ()))
    total[:, :WQ] += lax.dot_general(mixed_q, cq[...], lead, preferred_element_type=F32)
    total[:, WQ:] += lax.dot_general(mixed_v, cv[...], lead, preferred_element_type=F32)

    @pl.when(step == pl.num_programs(0) - 1)
    def _():
        major, _, per_major, per_minor = own_place()
        for offset, out in enumerate((own, to_1, to_2, to_3)):
            there = lax.rem(major + offset, 4)
            for minor in range(4):
                start = pl.multiple_of((there * per_major + minor * per_minor) * 16, 16)
                out[minor * 16 : (minor + 1) * 16, :] = total[pl.ds(start, 16), :].astype(out.dtype)


def projected_gradient(inputs, cq, cv, pq, pv, wq, wv):
    tokens, width = inputs.shape
    whole = lambda a: pl.BlockSpec(a.shape, lambda i: (0, 0))
    by_tokens = lambda a: pl.BlockSpec((TOKEN_BLOCK, a.shape[1]), lambda i: (i, 0))
    out = [
        jax.ShapeDtypeStruct((64, W), F32),
        jax.ShapeDtypeStruct((64, W), BF16),
        jax.ShapeDtypeStruct((64, W), BF16),
        jax.ShapeDtypeStruct((64, W), BF16),
        jax.ShapeDtypeStruct((ROWS, W), BF16),
    ]
    return pl.pallas_call(
        gradient_kernel,
        grid=(tokens // TOKEN_BLOCK,),
        in_specs=[by_tokens(inputs), by_tokens(cq), by_tokens(cv)]
        + [whole(a) for a in (pq, pv, wq, wv)],
        out_specs=[whole(a) for a in out],
        out_shape=[pltpu.VMEM(o.shape, o.dtype) for o in out],
        scratch_shapes=[pltpu.VMEM((RANK, W), F32)],
        cost_estimate=pl.CostEstimate(
            flops=2 * tokens * RANK * (2 * width + W), bytes_accessed=20_000_000, transcendentals=0
        ),
        compiler_params=pltpu.CompilerParams(vmem_limit_bytes=28 * 2**20),
        name="gradient",
    )(*(pltpu.with_memory_space_constraint(a, pltpu.HBM) for a in (inputs, cq, cv, pq, pv, wq, wv)))


def whole_call(body, out, operands, scratch=(), flops=1_000_000):
    vmem = pl.BlockSpec(memory_space=pltpu.VMEM)
    return pl.pallas_call(
        body,
        in_specs=[vmem] * len(operands),
        out_specs=[vmem] * len(out),
        out_shape=[pltpu.VMEM(o.shape, o.dtype) for o in out],
        scratch_shapes=list(scratch),
        cost_estimate=pl.CostEstimate(flops=flops, bytes_accessed=1_000_000, transcendentals=0),
        compiler_params=pltpu.CompilerParams(vmem_limit_bytes=8 * 2**20),
    )(*(in_vmem(a) for a in operands))


def partial_kernel(own, r1, r2, r3, mq, mv, vq, vv, out):
    out[:64, :] = (own[...] + r1[...].astype(F32) + (r2[...].astype(F32) + r3[...].astype(F32))).astype(BF16)
    out[64:80, :WQ] = mq[...].astype(BF16)
    out[64:80, WQ:] = mv[...].astype(BF16)
    out[80:96, :WQ] = vq[...].astype(BF16)
    out[80:96, WQ:] = vv[...].astype(BF16)


def moments(low, first, second):
    first_new = beta_first * first + (1.0 - beta_first) * low
    second_new = beta_second * second + (1.0 - beta_second) * low * low
    return first_new, second_new


def update_kernel(own, r1, r2, r3, mq, mv, vq, vv, u, fq, fv, sq, sv, low):
    low[...] = (own[:64, :].astype(F32) + r2[:64, :].astype(F32)) + (
        r1[:64, :].astype(F32) + r3[:64, :].astype(F32)
    )
    _, minor, _, _ = own_place()
    for offset, held in enumerate((own, r1, r2, r3)):
        there = lax.rem(minor + 4 - offset, 4)
        at = pl.ds(pl.multiple_of(there * 16, 16), 16)
        first, second = moments(low[at, :], held[64:80, :].astype(F32), held[80:96, :].astype(F32))
        u[at, :] = (first / (jnp.sqrt(second) + adam_eps)).astype(BF16)
    mine = low[pl.ds(pl.multiple_of(minor * 16, 16), 16), :]
    fq[...], sq[...] = moments(mine[:, :WQ], mq[...], vq[...])
    fv[...], sv[...] = moments(mine[:, WQ:], mv[...], vv[...])


def assemble_kernel(own, r1, r2, r3, u, squares):
    major, _, per_major, per_minor = own_place()
    for offset, held in enumerate((own, r1, r2, r3)):
        there = lax.rem(major + 4 - offset, 4)
        for minor in range(4):
            start = pl.multiple_of((there * per_major + minor * per_minor) * 16, 16)
            u[pl.ds(start, 16), :] = held[minor * 16 : (minor + 1) * 16, :]
    total = jnp.zeros((16, W), F32)
    for group in range(16):
        part = u[group * 16 : (group + 1) * 16, :].astype(F32)
        total += part * part
    total = total[:8, :] + total[8:, :]
    folded = total[:, :128]
    for lane in range(1, W // 128):
        folded += total[:, lane * 128 : (lane + 1) * 128]
    squares[...] = folded


def weight_kernel(
    s_own, s_other, u, pq, pv, g0, g1, g3, h_up, h_down, wq, wv,
    nq, nv, tq, tv, cq, cv, cq_s, cv_s, c_sem,
):
    major, minor, per_major, per_minor = own_place()
    squares = jnp.sum(s_own[...] + s_other[...], axis=(0, 1), keepdims=True)
    scale = lax.rsqrt(squares / (RANK * (QK_W + V_W)) + norm_eps)
    uq, uv = u[:, :WQ], u[:, WQ:]
    keep = 1.0 - step_rate * decay_rate
    stores = []
    for i, pieces in ((0, (g0, g0)), (1, (g1, g1)), (3, (g3, g3)), (2, (h_up, h_down))):
        b_there = lax.rem(minor + 4 - i, 4)
        for j in range(4):
            a_there = lax.rem(major + 4 - j, 4)
            block = a_there * per_major + b_there * per_minor
            at = pl.ds(pl.multiple_of(block * ROWS, ROWS), ROWS)
            back_q = scale * jnp.dot(pq[at, :], uq, preferred_element_type=F32)
            back_v = scale * jnp.dot(pv[at, :], uv, preferred_element_type=F32)
            piece = pieces[j // 2]
            top = (j if piece.shape[0] == 4 * ROWS else j % 2) * ROWS
            held = piece[top : top + ROWS, :].astype(F32)
            n = i * 4 + j
            cq_s[n] = (keep * held[:, :WQ] - step_rate * back_q).astype(BF16)
            cv_s[n] = (keep * held[:, WQ:] - step_rate * back_v).astype(BF16)
            for part, (source, target) in enumerate(((cq_s, cq), (cv_s, cv))):
                copy = pltpu.make_async_copy(source.at[n], target.at[at, :], c_sem.at[n, part])
                copy.start()
                stores.append(copy)
            if n == 0:
                for back, w, t, new in ((back_q, wq, tq, nq), (back_v, wv, tv, nv)):
                    weight = w[...]
                    step = back + decay_rate * weight
                    t[...] = step
                    new[...] = weight - step_rate * step
    for copy in stores:
        copy.wait()


def new_weights(s_own, s_other, u, pq, pv, groups, wq, wv):
    vmem = pl.BlockSpec(memory_space=pltpu.VMEM)
    hbm = pl.BlockSpec(memory_space=pl.ANY)
    out = [
        jax.ShapeDtypeStruct((ROWS, WQ), F32),
        jax.ShapeDtypeStruct((ROWS, WV), F32),
        jax.ShapeDtypeStruct((ROWS, WQ), F32),
        jax.ShapeDtypeStruct((ROWS, WV), F32),
        jax.ShapeDtypeStruct((16 * ROWS, WQ), BF16),
        jax.ShapeDtypeStruct((16 * ROWS, WV), BF16),
    ]
    operands = (s_own, s_other, u, pq, pv, *groups, wq, wv)
    return pl.pallas_call(
        weight_kernel,
        in_specs=[vmem] * len(operands),
        out_specs=[vmem] * 4 + [hbm] * 2,
        out_shape=out,
        scratch_shapes=[
            pltpu.VMEM((16, ROWS, WQ), BF16),
            pltpu.VMEM((16, ROWS, WV), BF16),
            pltpu.SemaphoreType.DMA((16, 2)),
        ],
        cost_estimate=pl.CostEstimate(
            flops=2 * 16 * ROWS * RANK * W, bytes_accessed=12_000_000, transcendentals=0
        ),
        compiler_params=pltpu.CompilerParams(vmem_limit_bytes=20 * 2**20),
        name="weights",
    )(*(in_vmem(a) for a in operands))


def on_device(inputs, cq, cv, pq, pv, wq, wv, mq, mv, vq, vv):
    own, to_1, to_2, to_3, w16 = projected_gradient(inputs, cq, cv, pq, pv, wq, wv)
    r_2, r_1, r_3 = (shifted(a, "major", n) for n, a in ((2, to_2), (1, to_1), (3, to_3)))
    w_1, w_3, w_2 = (shifted(w16, "major", n) for n in (1, 3, 2))
    message, = whole_call(
        partial_kernel, [jax.ShapeDtypeStruct((96, W), BF16)], (own, r_1, r_2, r_3, mq, mv, vq, vv)
    )
    m_2, m_1, m_3 = (shifted(message, "minor", n) for n in (2, 1, 3))
    group = jnp.concatenate([w16, w_1, w_2, w_3], axis=0)
    g_1, g_3 = shifted(group, "minor", 1), shifted(group, "minor", 3)
    small = lambda n: jax.ShapeDtypeStruct((16, n), F32)
    u_own, first_q, first_v, second_q, second_v = whole_call(
        update_kernel,
        [jax.ShapeDtypeStruct((64, W), BF16), small(WQ), small(WV), small(WQ), small(WV)],
        (message, m_1, m_2, m_3, mq, mv, vq, vv),
        [pltpu.VMEM((64, W), F32)],
    )
    u_2, u_1, u_3 = (shifted(u_own, "major", n) for n in (2, 1, 3))
    u, squares = whole_call(
        assemble_kernel,
        [jax.ShapeDtypeStruct((RANK, W), BF16), jax.ShapeDtypeStruct((8, 128), F32)],
        (u_own, u_1, u_2, u_3),
    )
    s_2, s_1, s_3 = (shifted(squares, "x", n) for n in (2, 1, 3))
    h_up = shifted(g_1[: 2 * ROWS], "minor", 1)
    h_down = shifted(g_3[2 * ROWS :], "minor", 3)
    chips = (squares + s_2) + (s_1 + s_3)
    other = shifted(chips, "core", 1)
    new_q, new_v, step_q, step_v, copy_q, copy_v = new_weights(
        chips, other, u, pq, pv, (group, g_1, g_3, h_up, h_down), wq, wv
    )
    return (new_q, new_v, copy_q, copy_v, first_q, first_v, second_q, second_v, step_q, step_v)


def solution(mesh):
    finer = Mesh(mesh.devices.reshape(SIZES), AXES)
    both, tokens, columns = P(FS, TP), P(FS, None), P(None, TP)
    return jax.shard_map(
        on_device,
        mesh=finer,
        in_specs=(tokens, both, both, P(), P()) + (both,) * 6,
        out_specs=(both, both, columns, columns) + (both,) * 6,
        check_vma=False,
    )
```

```python
import jax
import jax.numpy as jnp
from jax import lax
from jax.experimental import pallas as pl
from jax.experimental.pallas import tpu as pltpu
from jax.sharding import Mesh
from jax.sharding import PartitionSpec as P

RANK = 256
QK_W = 2048
V_W = 4096
AXES = ("z", "y", "x", "c")
SIZES = (4, 4, 4, 2)
FS = ("z", "y")
TP = ("x", "c")

beta_first = 0.9
beta_second = 0.95
adam_eps = 1e-08
norm_eps = 1e-06
step_rate = 0.05
decay_rate = 0.2

WQ = 256
WV = 512
W = WQ + WV
ROWS = 128
TOKEN_BLOCK = 1024

F32 = jnp.float32
BF16 = jnp.bfloat16


def shift_pairs(kind, offset):
    pairs = []
    for z in range(4):
        for y in range(4):
            for x in range(4):
                for c in range(2):
                    to = [z, y, x, c]
                    if kind == "major":
                        axis = 0 if c == 0 else 1
                    elif kind == "minor":
                        axis = 1 if c == 0 else 0
                    elif kind == "x":
                        axis = 2
                    else:
                        axis = 3
                    to[axis] = (to[axis] + offset) % SIZES[axis]
                    source = ((z * 4 + y) * 4 + x) * 2 + c
                    target = ((to[0] * 4 + to[1]) * 4 + to[2]) * 2 + to[3]
                    pairs.append((source, target))
    return pairs


def shifted(array, kind, offset):
    return lax.ppermute(array, AXES, shift_pairs(kind, offset))


def own_place():
    z, y, c = lax.axis_index("z"), lax.axis_index("y"), lax.axis_index("c")
    first = c == 0
    major = jnp.where(first, z, y)
    minor = jnp.where(first, y, z)
    per_major = jnp.where(first, 4, 1)
    per_minor = jnp.where(first, 1, 4)
    return major, minor, per_major, per_minor


def in_vmem(array):
    return pltpu.with_memory_space_constraint(array, pltpu.VMEM)


def in_hbm(array):
    return pltpu.with_memory_space_constraint(array, pltpu.HBM)


def prepare_kernel(wq, wv, pq, pv, w16, pq_out, pv_out, wq_s, wv_s, sem):
    pairs = ((wq, wq_s), (wv, wv_s), (pq, pq_out), (pv, pv_out))
    loads = [pltpu.make_async_copy(a, b, sem.at[n]) for n, (a, b) in enumerate(pairs)]
    for copy in loads:
        copy.start()
    loads[0].wait()
    w16[:, :WQ] = wq_s[...].astype(BF16)
    loads[1].wait()
    w16[:, WQ:] = wv_s[...].astype(BF16)
    loads[2].wait()
    loads[3].wait()


def prepare(wq, wv, pq, pv):
    vmem = pl.BlockSpec(memory_space=pltpu.VMEM)
    return pl.pallas_call(
        prepare_kernel,
        in_specs=[pl.BlockSpec(memory_space=pl.ANY)] * 4,
        out_specs=[vmem] * 3,
        out_shape=[
            pltpu.VMEM((ROWS, W), BF16),
            pltpu.VMEM(pq.shape, BF16),
            pltpu.VMEM(pv.shape, BF16),
        ],
        scratch_shapes=[
            pltpu.VMEM(wq.shape, F32),
            pltpu.VMEM(wv.shape, F32),
            pltpu.SemaphoreType.DMA((4,)),
        ],
        cost_estimate=pl.CostEstimate(flops=1_000_000, bytes_accessed=3_000_000, transcendentals=0),
        compiler_params=pltpu.CompilerParams(vmem_limit_bytes=8 * 2**20),
        name="prepare",
    )(*(in_hbm(a) for a in (wq, wv, pq, pv)))


def gradient_kernel(x, cq, cv, pq, pv, own, to_1, to_2, to_3, total):
    step = pl.program_id(0)

    @pl.when(step == 0)
    def _():
        total[...] = jnp.zeros_like(total)

    rows = x[...]
    mixed_q = jnp.dot(rows, pq[...], preferred_element_type=F32).astype(BF16)
    mixed_v = jnp.dot(rows, pv[...], preferred_element_type=F32).astype(BF16)
    lead = (((0,), (0,)), ((), ()))
    total[:, :WQ] += lax.dot_general(mixed_q, cq[...], lead, preferred_element_type=F32)
    total[:, WQ:] += lax.dot_general(mixed_v, cv[...], lead, preferred_element_type=F32)

    @pl.when(step == pl.num_programs(0) - 1)
    def _():
        major, _, per_major, per_minor = own_place()
        for offset, out in enumerate((own, to_1, to_2, to_3)):
            there = lax.rem(major + offset, 4)
            for minor in range(4):
                start = pl.multiple_of((there * per_major + minor * per_minor) * 16, 16)
                out[minor * 16 : (minor + 1) * 16, :] = total[pl.ds(start, 16), :].astype(out.dtype)


def projected_gradient(inputs, cq, cv, pq, pv):
    tokens, width = inputs.shape
    vmem = pl.BlockSpec(memory_space=pltpu.VMEM)
    by_tokens = lambda a: pl.BlockSpec((TOKEN_BLOCK, a.shape[1]), lambda i: (i, 0))
    return pl.pallas_call(
        gradient_kernel,
        grid=(tokens // TOKEN_BLOCK,),
        in_specs=[by_tokens(inputs), by_tokens(cq), by_tokens(cv), vmem, vmem],
        out_specs=[vmem] * 4,
        out_shape=[pltpu.VMEM((64, W), F32)] + [pltpu.VMEM((64, W), BF16)] * 3,
        scratch_shapes=[pltpu.VMEM((RANK, W), F32)],
        cost_estimate=pl.CostEstimate(
            flops=2 * tokens * RANK * (2 * width + W), bytes_accessed=18_000_000, transcendentals=0
        ),
        compiler_params=pltpu.CompilerParams(vmem_limit_bytes=32 * 2**20),
        name="gradient",
    )(in_hbm(inputs), in_hbm(cq), in_hbm(cv), in_vmem(pq), in_vmem(pv))


def whole_call(body, out, operands, scratch=(), flops=1_000_000):
    vmem = pl.BlockSpec(memory_space=pltpu.VMEM)
    return pl.pallas_call(
        body,
        in_specs=[vmem] * len(operands),
        out_specs=[vmem] * len(out),
        out_shape=[pltpu.VMEM(o.shape, o.dtype) for o in out],
        scratch_shapes=list(scratch),
        cost_estimate=pl.CostEstimate(flops=flops, bytes_accessed=1_000_000, transcendentals=0),
        compiler_params=pltpu.CompilerParams(vmem_limit_bytes=8 * 2**20),
    )(*(in_vmem(a) for a in operands))


def partial_kernel(own, r1, r2, r3, mq, mv, vq, vv, out):
    out[:64, :] = (own[...] + r1[...].astype(F32) + (r2[...].astype(F32) + r3[...].astype(F32))).astype(BF16)
    out[64:80, :WQ] = mq[...].astype(BF16)
    out[64:80, WQ:] = mv[...].astype(BF16)
    out[80:96, :WQ] = vq[...].astype(BF16)
    out[80:96, WQ:] = vv[...].astype(BF16)


def moments(low, first, second):
    first_new = beta_first * first + (1.0 - beta_first) * low
    second_new = beta_second * second + (1.0 - beta_second) * low * low
    return first_new, second_new


def update_kernel(own, r1, r2, r3, mq, mv, vq, vv, u, fq, fv, sq, sv, low):
    low[...] = (own[:64, :].astype(F32) + r2[:64, :].astype(F32)) + (
        r1[:64, :].astype(F32) + r3[:64, :].astype(F32)
    )
    _, minor, _, _ = own_place()
    for offset, held in enumerate((own, r1, r2, r3)):
        there = lax.rem(minor + 4 - offset, 4)
        at = pl.ds(pl.multiple_of(there * 16, 16), 16)
        first, second = moments(low[at, :], held[64:80, :].astype(F32), held[80:96, :].astype(F32))
        u[at, :] = (first / (jnp.sqrt(second) + adam_eps)).astype(BF16)
    mine = low[pl.ds(pl.multiple_of(minor * 16, 16), 16), :]
    fq[...], sq[...] = moments(mine[:, :WQ], mq[...], vq[...])
    fv[...], sv[...] = moments(mine[:, WQ:], mv[...], vv[...])


def assemble_kernel(own, r1, r2, r3, u, squares):
    major, _, per_major, per_minor = own_place()
    for offset, held in enumerate((own, r1, r2, r3)):
        there = lax.rem(major + 4 - offset, 4)
        for minor in range(4):
            start = pl.multiple_of((there * per_major + minor * per_minor) * 16, 16)
            u[pl.ds(start, 16), :] = held[minor * 16 : (minor + 1) * 16, :]
    total = jnp.zeros((16, W), F32)
    for group in range(16):
        part = u[group * 16 : (group + 1) * 16, :].astype(F32)
        total += part * part
    total = total[:8, :] + total[8:, :]
    folded = total[:, :128]
    for lane in range(1, W // 128):
        folded += total[:, lane * 128 : (lane + 1) * 128]
    squares[...] = folded


def weight_kernel(
    s_own, s_other, u, pq, pv, g0, g1, g3, h_up, h_down, wq, wv, fq, fv, sq, sv,
    nq, nv, tq, tv, cq, cv, fq_out, fv_out, sq_out, sv_out,
    nq_s, nv_s, tq_s, tv_s, cq_s, cv_s, c_sem, m_sem,
):
    stores = []

    def store(source, target, sem):
        copy = pltpu.make_async_copy(source, target, sem)
        copy.start()
        stores.append(copy)

    for n, (a, b) in enumerate(((fq, fq_out), (fv, fv_out), (sq, sq_out), (sv, sv_out))):
        store(a, b, m_sem.at[n])
    major, minor, per_major, per_minor = own_place()
    squares = jnp.sum(s_own[...] + s_other[...], axis=(0, 1), keepdims=True)
    scale = lax.rsqrt(squares / (RANK * (QK_W + V_W)) + norm_eps)
    uq, uv = u[:, :WQ], u[:, WQ:]
    keep = 1.0 - step_rate * decay_rate
    for i, pieces in ((0, (g0, g0)), (1, (g1, g1)), (3, (g3, g3)), (2, (h_up, h_down))):
        a_there = lax.rem(major + 4 - i, 4)
        for j in range(4):
            b_there = lax.rem(minor + 4 - j, 4)
            block = a_there * per_major + b_there * per_minor
            at = pl.ds(pl.multiple_of(block * ROWS, ROWS), ROWS)
            back_q = scale * jnp.dot(pq[at, :], uq, preferred_element_type=F32)
            back_v = scale * jnp.dot(pv[at, :], uv, preferred_element_type=F32)
            piece = pieces[j // 2]
            top = (j if piece.shape[0] == 4 * ROWS else j % 2) * ROWS
            held = piece[top : top + ROWS, :].astype(F32)
            n = i * 4 + j
            cq_s[n] = (keep * held[:, :WQ] - step_rate * back_q).astype(BF16)
            cv_s[n] = (keep * held[:, WQ:] - step_rate * back_v).astype(BF16)
            for part, (source, target) in enumerate(((cq_s, cq), (cv_s, cv))):
                store(source.at[n], target.at[at, :], c_sem.at[n, part])
            if n == 0:
                for back, w, t, new in ((back_q, wq, tq_s, nq_s), (back_v, wv, tv_s, nv_s)):
                    weight = w[...]
                    step = back + decay_rate * weight
                    t[...] = step
                    new[...] = weight - step_rate * step
                for k, (a, b) in enumerate(((nq_s, nq), (nv_s, nv), (tq_s, tq), (tv_s, tv))):
                    store(a, b, m_sem.at[4 + k])
    for copy in stores:
        copy.wait()


def new_weights(s_own, s_other, u, pq, pv, groups, wq, wv, kept):
    vmem = pl.BlockSpec(memory_space=pltpu.VMEM)
    hbm = pl.BlockSpec(memory_space=pl.ANY)
    out = [
        jax.ShapeDtypeStruct((ROWS, WQ), F32),
        jax.ShapeDtypeStruct((ROWS, WV), F32),
        jax.ShapeDtypeStruct((ROWS, WQ), F32),
        jax.ShapeDtypeStruct((ROWS, WV), F32),
        jax.ShapeDtypeStruct((16 * ROWS, WQ), BF16),
        jax.ShapeDtypeStruct((16 * ROWS, WV), BF16),
    ] + [jax.ShapeDtypeStruct(a.shape, F32) for a in kept]
    operands = (s_own, s_other, u, pq, pv, *groups, wq, wv, *kept)
    return pl.pallas_call(
        weight_kernel,
        in_specs=[vmem] * len(operands),
        out_specs=[hbm] * len(out),
        out_shape=out,
        scratch_shapes=[
            pltpu.VMEM((ROWS, WQ), F32),
            pltpu.VMEM((ROWS, WV), F32),
            pltpu.VMEM((ROWS, WQ), F32),
            pltpu.VMEM((ROWS, WV), F32),
            pltpu.VMEM((16, ROWS, WQ), BF16),
            pltpu.VMEM((16, ROWS, WV), BF16),
            pltpu.SemaphoreType.DMA((16, 2)),
            pltpu.SemaphoreType.DMA((8,)),
        ],
        cost_estimate=pl.CostEstimate(
            flops=2 * 16 * ROWS * RANK * W, bytes_accessed=12_000_000, transcendentals=0
        ),
        compiler_params=pltpu.CompilerParams(vmem_limit_bytes=20 * 2**20),
        name="weights",
    )(*(in_vmem(a) for a in operands))


def on_device(inputs, cq, cv, pq, pv, wq, wv, mq, mv, vq, vv):
    w16, pq, pv = prepare(wq, wv, pq, pv)
    w_1, w_3, w_2 = (shifted(w16, "minor", n) for n in (1, 3, 2))
    own, to_1, to_2, to_3 = projected_gradient(inputs, cq, cv, pq, pv)
    r_2, r_1, r_3 = (shifted(a, "major", n) for n, a in ((2, to_2), (1, to_1), (3, to_3)))
    group = jnp.concatenate([w16, w_1, w_2, w_3], axis=0)
    g_1, g_3 = shifted(group, "major", 1), shifted(group, "major", 3)
    message, = whole_call(
        partial_kernel, [jax.ShapeDtypeStruct((96, W), BF16)], (own, r_1, r_2, r_3, mq, mv, vq, vv)
    )
    m_2, m_1, m_3 = (shifted(message, "minor", n) for n in (2, 1, 3))
    small = lambda n: jax.ShapeDtypeStruct((16, n), F32)
    u_own, first_q, first_v, second_q, second_v = whole_call(
        update_kernel,
        [jax.ShapeDtypeStruct((64, W), BF16), small(WQ), small(WV), small(WQ), small(WV)],
        (message, m_1, m_2, m_3, mq, mv, vq, vv),
        [pltpu.VMEM((64, W), F32)],
    )
    u_2, u_1, u_3 = (shifted(u_own, "major", n) for n in (2, 1, 3))
    h_up = shifted(g_1[: 2 * ROWS], "major", 1)
    h_down = shifted(g_3[2 * ROWS :], "major", 3)
    u, squares = whole_call(
        assemble_kernel,
        [jax.ShapeDtypeStruct((RANK, W), BF16), jax.ShapeDtypeStruct((8, 128), F32)],
        (u_own, u_1, u_2, u_3),
    )
    s_2, s_1, s_3 = (shifted(squares, "x", n) for n in (2, 1, 3))
    chips = (squares + s_2) + (s_1 + s_3)
    other = shifted(chips, "core", 1)
    kept = (first_q, first_v, second_q, second_v)
    new_q, new_v, step_q, step_v, copy_q, copy_v, *kept = new_weights(
        chips, other, u, pq, pv, (group, g_1, g_3, h_up, h_down), wq, wv, kept
    )
    return (new_q, new_v, copy_q, copy_v, *kept, step_q, step_v)


def solution(mesh):
    finer = Mesh(mesh.devices.reshape(SIZES), AXES)
    both, tokens, columns = P(FS, TP), P(FS, None), P(None, TP)
    return jax.shard_map(
        on_device,
        mesh=finer,
        in_specs=(tokens, both, both, P(), P()) + (both,) * 6,
        out_specs=(both, both, columns, columns) + (both,) * 6,
        check_vma=False,
    )
```

```python
import jax
import jax.numpy as jnp
from jax import lax
from jax.experimental import pallas as pl
from jax.experimental.pallas import tpu as pltpu
from jax.sharding import Mesh
from jax.sharding import PartitionSpec as P

RANK = 256
QK_W = 2048
V_W = 4096
AXES = ("z", "y", "x", "c")
SIZES = (4, 4, 4, 2)
FS = ("z", "y")
TP = ("x", "c")

beta_first = 0.9
beta_second = 0.95
adam_eps = 1e-08
norm_eps = 1e-06
step_rate = 0.05
decay_rate = 0.2

WQ = 256
WV = 512
W = WQ + WV
ROWS = 128
MESSAGE = ROWS + 32
FRONT = 1024
AHEAD = 512

F32 = jnp.float32
BF16 = jnp.bfloat16


def shift_pairs(kind, offset):
    pairs = []
    for z in range(4):
        for y in range(4):
            for x in range(4):
                for c in range(2):
                    to = [z, y, x, c]
                    if kind == "major":
                        axis = 0 if c == 0 else 1
                    elif kind == "minor":
                        axis = 1 if c == 0 else 0
                    elif kind == "x":
                        axis = 2
                    else:
                        axis = 3
                    to[axis] = (to[axis] + offset) % SIZES[axis]
                    source = ((z * 4 + y) * 4 + x) * 2 + c
                    target = ((to[0] * 4 + to[1]) * 4 + to[2]) * 2 + to[3]
                    pairs.append((source, target))
    return pairs


def shifted(array, kind, offset):
    return lax.ppermute(array, AXES, shift_pairs(kind, offset))


def own_place():
    z, y, c = lax.axis_index("z"), lax.axis_index("y"), lax.axis_index("c")
    first = c == 0
    major = jnp.where(first, z, y)
    minor = jnp.where(first, y, z)
    per_major = jnp.where(first, 4, 1)
    per_minor = jnp.where(first, 1, 4)
    return major, minor, per_major, per_minor


def in_vmem(array):
    return pltpu.with_memory_space_constraint(array, pltpu.VMEM)


def in_hbm(array):
    return pltpu.with_memory_space_constraint(array, pltpu.HBM)


def prepare_kernel(wq, wv, pq, pv, mq, mv, vq, vv, w16, pq_out, pv_out, wq_s, wv_s, m_s, v_s, sem):
    pairs = (
        (wq, wq_s),
        (wv, wv_s),
        (mq, m_s.at[:, pl.ds(0, WQ)]),
        (mv, m_s.at[:, pl.ds(WQ, WV)]),
        (vq, v_s.at[:, pl.ds(0, WQ)]),
        (vv, v_s.at[:, pl.ds(WQ, WV)]),
        (pq, pq_out),
        (pv, pv_out),
    )
    loads = [pltpu.make_async_copy(a, b, sem.at[n]) for n, (a, b) in enumerate(pairs)]
    for copy in loads:
        copy.start()
    for copy in loads[:6]:
        copy.wait()
    w16[:ROWS, :WQ] = wq_s[...].astype(BF16)
    w16[:ROWS, WQ:] = wv_s[...].astype(BF16)
    w16[ROWS : ROWS + 16, :] = m_s[...].astype(BF16)
    w16[ROWS + 16 :, :] = v_s[...].astype(BF16)
    for copy in loads[6:]:
        copy.wait()


def prepare(wq, wv, pq, pv, mq, mv, vq, vv):
    vmem = pl.BlockSpec(memory_space=pltpu.VMEM)
    return pl.pallas_call(
        prepare_kernel,
        in_specs=[pl.BlockSpec(memory_space=pl.ANY)] * 8,
        out_specs=[vmem] * 3,
        out_shape=[
            pltpu.VMEM((MESSAGE, W), BF16),
            pltpu.VMEM(pq.shape, BF16),
            pltpu.VMEM(pv.shape, BF16),
        ],
        scratch_shapes=[
            pltpu.VMEM(wq.shape, F32),
            pltpu.VMEM(wv.shape, F32),
            pltpu.VMEM((16, W), F32),
            pltpu.VMEM((16, W), F32),
            pltpu.SemaphoreType.DMA((8,)),
        ],
        cost_estimate=pl.CostEstimate(flops=1_000_000, bytes_accessed=3_000_000, transcendentals=0),
        compiler_params=pltpu.CompilerParams(vmem_limit_bytes=8 * 2**20),
        name="prepare",
    )(*(in_hbm(a) for a in (wq, wv, pq, pv, mq, mv, vq, vv)))


def products(x, cq, cv, pq, pv):
    lead = (((0,), (0,)), ((), ()))
    mixed_q = jnp.dot(x, pq[...], preferred_element_type=F32).astype(BF16)
    mixed_v = jnp.dot(x, pv[...], preferred_element_type=F32).astype(BF16)
    return (
        lax.dot_general(mixed_q, cq, lead, preferred_element_type=F32),
        lax.dot_general(mixed_v, cv, lead, preferred_element_type=F32),
    )


def block_copies(sources, targets, start, size, at, sem):
    return [
        pltpu.make_async_copy(a.at[pl.ds(start, size), :], b.at[pl.ds(at, size), :], sem.at[n])
        for n, (a, b) in enumerate(zip(sources, targets))
    ]


def front_kernel(x, cq, cv, pq, pv, total, xn, cqn, cvn, xs, cqs, cvs, sem):
    sources, half = (x, cq, cv), FRONT // 2
    blocks = [
        block_copies(sources, (xs, cqs, cvs), n * half, half, n * half, sem.at[n]) for n in range(2)
    ]
    later = block_copies(sources, (xn, cqn, cvn), FRONT, AHEAD, 0, sem.at[2])
    for copy in (*blocks[0], *blocks[1], *later):
        copy.start()
    for n in range(2):
        for copy in blocks[n]:
            copy.wait()
        at = slice(n * half, (n + 1) * half)
        part_q, part_v = products(xs[at, :], cqs[at, :], cvs[at, :], pq, pv)
        if n == 0:
            total[:, :WQ] = part_q
            total[:, WQ:] = part_v
        else:
            total[:, :WQ] += part_q
            total[:, WQ:] += part_v
    for copy in later:
        copy.wait()


def rest_kernel(
    x, cq, cv, pq, pv, so_far, xn, cqn, cvn, own, to_1, to_2, to_3, total, xs, cqs, cvs, sem
):
    sources, size = (x, cq, cv), xs.shape[0] // 2
    first = FRONT + AHEAD
    blocks = [
        block_copies(sources, (xs, cqs, cvs), first + n * size, size, n * size, sem.at[n])
        for n in range(2)
    ]
    for copy in (*blocks[0], *blocks[1]):
        copy.start()
    part_q, part_v = products(xn[...], cqn[...], cvn[...], pq, pv)
    total[:, :WQ] = so_far[:, :WQ] + part_q
    total[:, WQ:] = so_far[:, WQ:] + part_v
    for n in range(2):
        for copy in blocks[n]:
            copy.wait()
        at = slice(n * size, (n + 1) * size)
        part_q, part_v = products(xs[at, :], cqs[at, :], cvs[at, :], pq, pv)
        total[:, :WQ] += part_q
        total[:, WQ:] += part_v
    major, _, per_major, per_minor = own_place()
    for offset, out in enumerate((own, to_1, to_2, to_3)):
        there = lax.rem(major + offset, 4)
        for minor in range(4):
            start = pl.multiple_of((there * per_major + minor * per_minor) * 16, 16)
            out[minor * 16 : (minor + 1) * 16, :] = total[pl.ds(start, 16), :].astype(out.dtype)


def token_blocks(inputs, size):
    return [pltpu.VMEM((size, n), BF16) for n in (inputs.shape[1], WQ, WV)]


def product_call(body, arrays, held, out, scratch, tokens):
    vmem, hbm = pl.BlockSpec(memory_space=pltpu.VMEM), pl.BlockSpec(memory_space=pl.ANY)
    return pl.pallas_call(
        body,
        in_specs=[hbm] * 3 + [vmem] * len(held),
        out_specs=[vmem] * len(out),
        out_shape=out,
        scratch_shapes=scratch + [pltpu.SemaphoreType.DMA((3, 3))],
        cost_estimate=pl.CostEstimate(
            flops=2 * tokens * RANK * (2 * arrays[0].shape[1] + W),
            bytes_accessed=6_000 * tokens,
            transcendentals=0,
        ),
        compiler_params=pltpu.CompilerParams(vmem_limit_bytes=28 * 2**20),
    )(*(in_hbm(a) for a in arrays), *(in_vmem(a) for a in held))


def front_products(inputs, cq, cv, pq, pv):
    out = [pltpu.VMEM((RANK, W), F32)] + token_blocks(inputs, AHEAD)
    return product_call(
        front_kernel, (inputs, cq, cv), (pq, pv), out, token_blocks(inputs, FRONT), FRONT
    )


def rest_products(inputs, cq, cv, pq, pv, so_far, ahead):
    left = inputs.shape[0] - FRONT - AHEAD
    out = [pltpu.VMEM((64, W), F32)] + [pltpu.VMEM((64, W), BF16)] * 3
    scratch = [pltpu.VMEM((RANK, W), F32)] + token_blocks(inputs, left)
    held = (pq, pv, so_far, *ahead)
    return product_call(rest_kernel, (inputs, cq, cv), held, out, scratch, left + AHEAD)


def whole_call(body, out, operands, scratch=(), flops=1_000_000):
    vmem = pl.BlockSpec(memory_space=pltpu.VMEM)
    return pl.pallas_call(
        body,
        in_specs=[vmem] * len(operands),
        out_specs=[vmem] * len(out),
        out_shape=[pltpu.VMEM(o.shape, o.dtype) for o in out],
        scratch_shapes=list(scratch),
        cost_estimate=pl.CostEstimate(flops=flops, bytes_accessed=1_000_000, transcendentals=0),
        compiler_params=pltpu.CompilerParams(vmem_limit_bytes=8 * 2**20),
    )(*(in_vmem(a) for a in operands))


def group_kernel(w0, w1, w2, w3, after, out):
    for n, held in enumerate((w0, w1, w2, w3)):
        out[n * ROWS : (n + 1) * ROWS, :] = held[:ROWS, :]


def partial_kernel(own, r1, r2, r3, out):
    out[...] = (own[...] + r1[...].astype(F32) + (r2[...].astype(F32) + r3[...].astype(F32))).astype(BF16)


def moments(low, first, second):
    first_new = beta_first * first + (1.0 - beta_first) * low
    second_new = beta_second * second + (1.0 - beta_second) * low * low
    return first_new, second_new


def update_kernel(own, r1, r2, r3, k0, k1, k2, k3, mq, mv, vq, vv, u, fq, fv, sq, sv, low):
    low[...] = (own[...].astype(F32) + r2[...].astype(F32)) + (r1[...].astype(F32) + r3[...].astype(F32))
    _, minor, _, _ = own_place()
    for offset, held in enumerate((k0, k1, k2, k3)):
        there = lax.rem(minor + 4 - offset, 4)
        at = pl.ds(pl.multiple_of(there * 16, 16), 16)
        first = held[ROWS : ROWS + 16, :].astype(F32)
        second = held[ROWS + 16 :, :].astype(F32)
        first, second = moments(low[at, :], first, second)
        u[at, :] = (first / (jnp.sqrt(second) + adam_eps)).astype(BF16)
    mine = low[pl.ds(pl.multiple_of(minor * 16, 16), 16), :]
    fq[...], sq[...] = moments(mine[:, :WQ], mq[...], vq[...])
    fv[...], sv[...] = moments(mine[:, WQ:], mv[...], vv[...])


def assemble_kernel(own, r1, r2, r3, u, squares):
    major, _, per_major, per_minor = own_place()
    for offset, held in enumerate((own, r1, r2, r3)):
        there = lax.rem(major + 4 - offset, 4)
        for minor in range(4):
            start = pl.multiple_of((there * per_major + minor * per_minor) * 16, 16)
            u[pl.ds(start, 16), :] = held[minor * 16 : (minor + 1) * 16, :]
    total = jnp.zeros((16, W), F32)
    for group in range(16):
        part = u[group * 16 : (group + 1) * 16, :].astype(F32)
        total += part * part
    total = total[:8, :] + total[8:, :]
    folded = total[:, :128]
    for lane in range(1, W // 128):
        folded += total[:, lane * 128 : (lane + 1) * 128]
    squares[...] = folded


def weight_kernel(
    s_own, s_other, u, pq, pv, g0, g1, g3, h_up, h_down, wq, wv, fq, fv, sq, sv,
    nq, nv, tq, tv, cq, cv, fq_out, fv_out, sq_out, sv_out,
    nq_s, nv_s, tq_s, tv_s, cq_s, cv_s, c_sem, m_sem,
):
    stores = []

    def store(source, target, sem):
        copy = pltpu.make_async_copy(source, target, sem)
        copy.start()
        stores.append(copy)

    for n, (a, b) in enumerate(((fq, fq_out), (fv, fv_out), (sq, sq_out), (sv, sv_out))):
        store(a, b, m_sem.at[n])
    major, minor, per_major, per_minor = own_place()
    squares = jnp.sum(s_own[...] + s_other[...], axis=(0, 1), keepdims=True)
    scale = lax.rsqrt(squares / (RANK * (QK_W + V_W)) + norm_eps)
    uq, uv = u[:, :WQ], u[:, WQ:]
    keep = 1.0 - step_rate * decay_rate
    for i, pieces in ((0, (g0, g0)), (1, (g1, g1)), (3, (g3, g3)), (2, (h_up, h_down))):
        a_there = lax.rem(major + 4 - i, 4)
        for j in range(4):
            b_there = lax.rem(minor + 4 - j, 4)
            block = a_there * per_major + b_there * per_minor
            at = pl.ds(pl.multiple_of(block * ROWS, ROWS), ROWS)
            back_q = scale * jnp.dot(pq[at, :], uq, preferred_element_type=F32)
            back_v = scale * jnp.dot(pv[at, :], uv, preferred_element_type=F32)
            piece = pieces[j // 2]
            top = (j if piece.shape[0] == 4 * ROWS else j % 2) * ROWS
            held = piece[top : top + ROWS, :].astype(F32)
            n = i * 4 + j
            cq_s[n] = (keep * held[:, :WQ] - step_rate * back_q).astype(BF16)
            cv_s[n] = (keep * held[:, WQ:] - step_rate * back_v).astype(BF16)
            for part, (source, target) in enumerate(((cq_s, cq), (cv_s, cv))):
                store(source.at[n], target.at[at, :], c_sem.at[n, part])
            if n == 0:
                for back, w, t, new in ((back_q, wq, tq_s, nq_s), (back_v, wv, tv_s, nv_s)):
                    weight = w[...]
                    step = back + decay_rate * weight
                    t[...] = step
                    new[...] = weight - step_rate * step
                for k, (a, b) in enumerate(((nq_s, nq), (nv_s, nv), (tq_s, tq), (tv_s, tv))):
                    store(a, b, m_sem.at[4 + k])
    for copy in stores:
        copy.wait()


def new_weights(s_own, s_other, u, pq, pv, groups, wq, wv, kept):
    vmem = pl.BlockSpec(memory_space=pltpu.VMEM)
    hbm = pl.BlockSpec(memory_space=pl.ANY)
    out = [
        jax.ShapeDtypeStruct((ROWS, WQ), F32),
        jax.ShapeDtypeStruct((ROWS, WV), F32),
        jax.ShapeDtypeStruct((ROWS, WQ), F32),
        jax.ShapeDtypeStruct((ROWS, WV), F32),
        jax.ShapeDtypeStruct((16 * ROWS, WQ), BF16),
        jax.ShapeDtypeStruct((16 * ROWS, WV), BF16),
    ] + [jax.ShapeDtypeStruct(a.shape, F32) for a in kept]
    operands = (s_own, s_other, u, pq, pv, *groups, wq, wv, *kept)
    return pl.pallas_call(
        weight_kernel,
        in_specs=[vmem] * len(operands),
        out_specs=[hbm] * len(out),
        out_shape=out,
        scratch_shapes=[
            pltpu.VMEM((ROWS, WQ), F32),
            pltpu.VMEM((ROWS, WV), F32),
            pltpu.VMEM((ROWS, WQ), F32),
            pltpu.VMEM((ROWS, WV), F32),
            pltpu.VMEM((16, ROWS, WQ), BF16),
            pltpu.VMEM((16, ROWS, WV), BF16),
            pltpu.SemaphoreType.DMA((16, 2)),
            pltpu.SemaphoreType.DMA((8,)),
        ],
        cost_estimate=pl.CostEstimate(
            flops=2 * 16 * ROWS * RANK * W, bytes_accessed=12_000_000, transcendentals=0
        ),
        compiler_params=pltpu.CompilerParams(vmem_limit_bytes=20 * 2**20),
        name="weights",
    )(*(in_vmem(a) for a in operands))


def on_device(inputs, cq, cv, pq, pv, wq, wv, mq, mv, vq, vv):
    w16, pq, pv = prepare(wq, wv, pq, pv, mq, mv, vq, vv)
    w_2, w_1, w_3 = (shifted(w16, "minor", n) for n in (2, 1, 3))
    so_far, *ahead = front_products(inputs, cq, cv, pq, pv)
    group, = whole_call(
        group_kernel, [jax.ShapeDtypeStruct((4 * ROWS, W), BF16)], (w16, w_1, w_2, w_3, so_far)
    )
    g_1, g_3 = shifted(group, "major", 1), shifted(group, "major", 3)
    own, to_1, to_2, to_3 = rest_products(inputs, cq, cv, pq, pv, so_far, ahead)
    r_2, r_1, r_3 = (shifted(a, "major", n) for n, a in ((2, to_2), (1, to_1), (3, to_3)))
    message, = whole_call(
        partial_kernel, [jax.ShapeDtypeStruct((64, W), BF16)], (own, r_1, r_2, r_3)
    )
    m_2, m_1, m_3 = (shifted(message, "minor", n) for n in (2, 1, 3))
    h_up = shifted(g_1[: 2 * ROWS], "major", 1)
    h_down = shifted(g_3[2 * ROWS :], "major", 3)
    small = lambda n: jax.ShapeDtypeStruct((16, n), F32)
    u_own, first_q, first_v, second_q, second_v = whole_call(
        update_kernel,
        [jax.ShapeDtypeStruct((64, W), BF16), small(WQ), small(WV), small(WQ), small(WV)],
        (message, m_1, m_2, m_3, w16, w_1, w_2, w_3, mq, mv, vq, vv),
        [pltpu.VMEM((64, W), F32)],
    )
    u_2, u_1, u_3 = (shifted(u_own, "major", n) for n in (2, 1, 3))
    u, squares = whole_call(
        assemble_kernel,
        [jax.ShapeDtypeStruct((RANK, W), BF16), jax.ShapeDtypeStruct((8, 128), F32)],
        (u_own, u_1, u_2, u_3),
    )
    s_2, s_1, s_3 = (shifted(squares, "x", n) for n in (2, 1, 3))
    chips = (squares + s_2) + (s_1 + s_3)
    other = shifted(chips, "core", 1)
    kept = (first_q, first_v, second_q, second_v)
    new_q, new_v, step_q, step_v, copy_q, copy_v, *kept = new_weights(
        chips, other, u, pq, pv, (group, g_1, g_3, h_up, h_down), wq, wv, kept
    )
    return (new_q, new_v, copy_q, copy_v, *kept, step_q, step_v)


def solution(mesh):
    finer = Mesh(mesh.devices.reshape(SIZES), AXES)
    both, tokens, columns = P(FS, TP), P(FS, None), P(None, TP)
    return jax.shard_map(
        on_device,
        mesh=finer,
        in_specs=(tokens, both, both, P(), P()) + (both,) * 6,
        out_specs=(both, both, columns, columns) + (both,) * 6,
        check_vma=False,
    )
```

```python
import jax
import jax.numpy as jnp
from jax import lax
from jax.experimental import pallas as pl
from jax.experimental.pallas import tpu as pltpu
from jax.sharding import Mesh
from jax.sharding import PartitionSpec as P

RANK = 256
QK_W = 2048
V_W = 4096
AXES = ("z", "y", "x", "c")
SIZES = (4, 4, 4, 2)
FS = ("z", "y")
TP = ("x", "c")

beta_first = 0.9
beta_second = 0.95
adam_eps = 1e-08
norm_eps = 1e-06
step_rate = 0.05
decay_rate = 0.2

WQ = 256
WV = 512
W = WQ + WV
ROWS = 128
MESSAGE = ROWS + 32
TOKEN_BLOCK = 1024

F32 = jnp.float32
BF16 = jnp.bfloat16


def shift_pairs(kind, offset):
    pairs = []
    for z in range(4):
        for y in range(4):
            for x in range(4):
                for c in range(2):
                    to = [z, y, x, c]
                    if kind == "major":
                        axis = 0 if c == 0 else 1
                    elif kind == "minor":
                        axis = 1 if c == 0 else 0
                    elif kind == "x":
                        axis = 2
                    else:
                        axis = 3
                    to[axis] = (to[axis] + offset) % SIZES[axis]
                    source = ((z * 4 + y) * 4 + x) * 2 + c
                    target = ((to[0] * 4 + to[1]) * 4 + to[2]) * 2 + to[3]
                    pairs.append((source, target))
    return pairs


def shifted(array, kind, offset):
    return lax.ppermute(array, AXES, shift_pairs(kind, offset))


def to_all(kind, arrays):
    two = shifted(arrays[1], kind, 2)
    return shifted(arrays[0], kind, 1), two, shifted(arrays[2], kind, 3)


def own_place():
    z, y, c = lax.axis_index("z"), lax.axis_index("y"), lax.axis_index("c")
    first = c == 0
    major = jnp.where(first, z, y)
    minor = jnp.where(first, y, z)
    per_major = jnp.where(first, 4, 1)
    per_minor = jnp.where(first, 1, 4)
    return major, minor, per_major, per_minor


def in_vmem(array):
    return pltpu.with_memory_space_constraint(array, pltpu.VMEM)


def in_hbm(array):
    return pltpu.with_memory_space_constraint(array, pltpu.HBM)


def prepare_kernel(wq, wv, pq, pv, mq, mv, vq, vv, w16, pq_out, pv_out, wq_s, wv_s, m_s, v_s, sem):
    pairs = (
        (wq, wq_s),
        (wv, wv_s),
        (mq, m_s.at[:, pl.ds(0, WQ)]),
        (mv, m_s.at[:, pl.ds(WQ, WV)]),
        (vq, v_s.at[:, pl.ds(0, WQ)]),
        (vv, v_s.at[:, pl.ds(WQ, WV)]),
        (pq, pq_out),
        (pv, pv_out),
    )
    loads = [pltpu.make_async_copy(a, b, sem.at[n]) for n, (a, b) in enumerate(pairs)]
    for copy in loads:
        copy.start()
    for copy in loads[:6]:
        copy.wait()
    w16[:ROWS, :WQ] = wq_s[...].astype(BF16)
    w16[:ROWS, WQ:] = wv_s[...].astype(BF16)
    w16[ROWS : ROWS + 16, :] = m_s[...].astype(BF16)
    w16[ROWS + 16 :, :] = v_s[...].astype(BF16)
    for copy in loads[6:]:
        copy.wait()


def prepare(wq, wv, pq, pv, mq, mv, vq, vv):
    vmem = pl.BlockSpec(memory_space=pltpu.VMEM)
    return pl.pallas_call(
        prepare_kernel,
        in_specs=[pl.BlockSpec(memory_space=pl.ANY)] * 8,
        out_specs=[vmem] * 3,
        out_shape=[
            pltpu.VMEM((MESSAGE, W), BF16),
            pltpu.VMEM(pq.shape, BF16),
            pltpu.VMEM(pv.shape, BF16),
        ],
        scratch_shapes=[
            pltpu.VMEM(wq.shape, F32),
            pltpu.VMEM(wv.shape, F32),
            pltpu.VMEM((16, W), F32),
            pltpu.VMEM((16, W), F32),
            pltpu.SemaphoreType.DMA((8,)),
        ],
        cost_estimate=pl.CostEstimate(flops=1_000_000, bytes_accessed=3_000_000, transcendentals=0),
        compiler_params=pltpu.CompilerParams(vmem_limit_bytes=8 * 2**20),
        name="prepare",
    )(*(in_hbm(a) for a in (wq, wv, pq, pv, mq, mv, vq, vv)))


def gradient_kernel(x, cq, cv, pq, pv, own, to_1, to_2, to_3, total):
    step = pl.program_id(0)

    @pl.when(step == 0)
    def _():
        total[...] = jnp.zeros_like(total)

    rows = x[...]
    mixed_q = jnp.dot(rows, pq[...], preferred_element_type=F32).astype(BF16)
    mixed_v = jnp.dot(rows, pv[...], preferred_element_type=F32).astype(BF16)
    lead = (((0,), (0,)), ((), ()))
    total[:, :WQ] += lax.dot_general(mixed_q, cq[...], lead, preferred_element_type=F32)
    total[:, WQ:] += lax.dot_general(mixed_v, cv[...], lead, preferred_element_type=F32)

    @pl.when(step == pl.num_programs(0) - 1)
    def _():
        major, _, per_major, per_minor = own_place()
        for offset, out in enumerate((own, to_1, to_2, to_3)):
            there = lax.rem(major + offset, 4)
            for minor in range(4):
                start = pl.multiple_of((there * per_major + minor * per_minor) * 16, 16)
                out[minor * 16 : (minor + 1) * 16, :] = total[pl.ds(start, 16), :].astype(out.dtype)


def projected_gradient(inputs, cq, cv, pq, pv):
    tokens, width = inputs.shape
    vmem = pl.BlockSpec(memory_space=pltpu.VMEM)
    by_tokens = lambda a: pl.BlockSpec((TOKEN_BLOCK, a.shape[1]), lambda i: (i, 0))
    return pl.pallas_call(
        gradient_kernel,
        grid=(tokens // TOKEN_BLOCK,),
        in_specs=[by_tokens(inputs), by_tokens(cq), by_tokens(cv), vmem, vmem],
        out_specs=[vmem] * 4,
        out_shape=[pltpu.VMEM((64, W), F32)] + [pltpu.VMEM((64, W), BF16)] * 3,
        scratch_shapes=[pltpu.VMEM((RANK, W), F32)],
        cost_estimate=pl.CostEstimate(
            flops=2 * tokens * RANK * (2 * width + W), bytes_accessed=18_000_000, transcendentals=0
        ),
        compiler_params=pltpu.CompilerParams(vmem_limit_bytes=32 * 2**20),
        name="gradient",
    )(in_hbm(inputs), in_hbm(cq), in_hbm(cv), in_vmem(pq), in_vmem(pv))


def whole_call(body, out, operands, scratch=(), flops=1_000_000):
    vmem = pl.BlockSpec(memory_space=pltpu.VMEM)
    return pl.pallas_call(
        body,
        in_specs=[vmem] * len(operands),
        out_specs=[vmem] * len(out),
        out_shape=[pltpu.VMEM(o.shape, o.dtype) for o in out],
        scratch_shapes=list(scratch),
        cost_estimate=pl.CostEstimate(flops=flops, bytes_accessed=1_000_000, transcendentals=0),
        compiler_params=pltpu.CompilerParams(vmem_limit_bytes=8 * 2**20),
    )(*(in_vmem(a) for a in operands))


def group_kernel(w0, w1, w2, w3, out):
    for n, held in enumerate((w0, w1, w2, w3)):
        out[n * ROWS : (n + 1) * ROWS, :] = held[:ROWS, :]


def partial_kernel(own, r1, r2, r3, out):
    out[...] = (own[...] + r1[...].astype(F32) + (r2[...].astype(F32) + r3[...].astype(F32))).astype(BF16)


def moments(low, first, second):
    first_new = beta_first * first + (1.0 - beta_first) * low
    second_new = beta_second * second + (1.0 - beta_second) * low * low
    return first_new, second_new


def update_kernel(own, r1, r2, r3, k0, k1, k2, k3, mq, mv, vq, vv, u, fq, fv, sq, sv, low):
    low[...] = (own[...].astype(F32) + r2[...].astype(F32)) + (r1[...].astype(F32) + r3[...].astype(F32))
    _, minor, _, _ = own_place()
    for offset, held in enumerate((k0, k1, k2, k3)):
        there = lax.rem(minor + 4 - offset, 4)
        at = pl.ds(pl.multiple_of(there * 16, 16), 16)
        first = held[ROWS : ROWS + 16, :].astype(F32)
        second = held[ROWS + 16 :, :].astype(F32)
        first, second = moments(low[at, :], first, second)
        u[at, :] = (first / (jnp.sqrt(second) + adam_eps)).astype(BF16)
    mine = low[pl.ds(pl.multiple_of(minor * 16, 16), 16), :]
    fq[...], sq[...] = moments(mine[:, :WQ], mq[...], vq[...])
    fv[...], sv[...] = moments(mine[:, WQ:], mv[...], vv[...])


def assemble_kernel(own, r1, r2, r3, u, squares):
    major, _, per_major, per_minor = own_place()
    for offset, held in enumerate((own, r1, r2, r3)):
        there = lax.rem(major + 4 - offset, 4)
        for minor in range(4):
            start = pl.multiple_of((there * per_major + minor * per_minor) * 16, 16)
            u[pl.ds(start, 16), :] = held[minor * 16 : (minor + 1) * 16, :]
    total = jnp.zeros((16, W), F32)
    for group in range(16):
        part = u[group * 16 : (group + 1) * 16, :].astype(F32)
        total += part * part
    total = total[:8, :] + total[8:, :]
    folded = total[:, :128]
    for lane in range(1, W // 128):
        folded += total[:, lane * 128 : (lane + 1) * 128]
    squares[...] = folded


def weight_kernel(
    s_own, s_other, u, pq, pv, g0, g1, g3, h_up, h_down, wq, wv, fq, fv, sq, sv,
    nq, nv, tq, tv, cq, cv, fq_out, fv_out, sq_out, sv_out,
    nq_s, nv_s, tq_s, tv_s, cq_s, cv_s, c_sem, m_sem,
):
    stores = []

    def store(source, target, sem):
        copy = pltpu.make_async_copy(source, target, sem)
        copy.start()
        stores.append(copy)

    for n, (a, b) in enumerate(((fq, fq_out), (fv, fv_out), (sq, sq_out), (sv, sv_out))):
        store(a, b, m_sem.at[n])
    major, minor, per_major, per_minor = own_place()
    squares = jnp.sum(s_own[...] + s_other[...], axis=(0, 1), keepdims=True)
    scale = lax.rsqrt(squares / (RANK * (QK_W + V_W)) + norm_eps)
    uq, uv = u[:, :WQ], u[:, WQ:]
    keep = 1.0 - step_rate * decay_rate
    for i, pieces in ((0, (g0, g0)), (1, (g1, g1)), (3, (g3, g3)), (2, (h_up, h_down))):
        a_there = lax.rem(major + 4 - i, 4)
        for j in range(4):
            b_there = lax.rem(minor + 4 - j, 4)
            block = a_there * per_major + b_there * per_minor
            at = pl.ds(pl.multiple_of(block * ROWS, ROWS), ROWS)
            back_q = scale * jnp.dot(pq[at, :], uq, preferred_element_type=F32)
            back_v = scale * jnp.dot(pv[at, :], uv, preferred_element_type=F32)
            piece = pieces[j // 2]
            top = (j if piece.shape[0] == 4 * ROWS else j % 2) * ROWS
            held = piece[top : top + ROWS, :].astype(F32)
            n = i * 4 + j
            cq_s[n] = (keep * held[:, :WQ] - step_rate * back_q).astype(BF16)
            cv_s[n] = (keep * held[:, WQ:] - step_rate * back_v).astype(BF16)
            for part, (source, target) in enumerate(((cq_s, cq), (cv_s, cv))):
                store(source.at[n], target.at[at, :], c_sem.at[n, part])
            if n == 0:
                for back, w, t, new in ((back_q, wq, tq_s, nq_s), (back_v, wv, tv_s, nv_s)):
                    weight = w[...]
                    step = back + decay_rate * weight
                    t[...] = step
                    new[...] = weight - step_rate * step
                for k, (a, b) in enumerate(((nq_s, nq), (nv_s, nv), (tq_s, tq), (tv_s, tv))):
                    store(a, b, m_sem.at[4 + k])
    for copy in stores:
        copy.wait()


def new_weights(s_own, s_other, u, pq, pv, groups, wq, wv, kept):
    vmem = pl.BlockSpec(memory_space=pltpu.VMEM)
    hbm = pl.BlockSpec(memory_space=pl.ANY)
    out = [
        jax.ShapeDtypeStruct((ROWS, WQ), F32),
        jax.ShapeDtypeStruct((ROWS, WV), F32),
        jax.ShapeDtypeStruct((ROWS, WQ), F32),
        jax.ShapeDtypeStruct((ROWS, WV), F32),
        jax.ShapeDtypeStruct((16 * ROWS, WQ), BF16),
        jax.ShapeDtypeStruct((16 * ROWS, WV), BF16),
    ] + [jax.ShapeDtypeStruct(a.shape, F32) for a in kept]
    operands = (s_own, s_other, u, pq, pv, *groups, wq, wv, *kept)
    return pl.pallas_call(
        weight_kernel,
        in_specs=[vmem] * len(operands),
        out_specs=[hbm] * len(out),
        out_shape=out,
        scratch_shapes=[
            pltpu.VMEM((ROWS, WQ), F32),
            pltpu.VMEM((ROWS, WV), F32),
            pltpu.VMEM((ROWS, WQ), F32),
            pltpu.VMEM((ROWS, WV), F32),
            pltpu.VMEM((16, ROWS, WQ), BF16),
            pltpu.VMEM((16, ROWS, WV), BF16),
            pltpu.SemaphoreType.DMA((16, 2)),
            pltpu.SemaphoreType.DMA((8,)),
        ],
        cost_estimate=pl.CostEstimate(
            flops=2 * 16 * ROWS * RANK * W, bytes_accessed=12_000_000, transcendentals=0
        ),
        compiler_params=pltpu.CompilerParams(vmem_limit_bytes=20 * 2**20),
        name="weights",
    )(*(in_vmem(a) for a in operands))


def on_device(inputs, cq, cv, pq, pv, wq, wv, mq, mv, vq, vv):
    w16, pq, pv = prepare(wq, wv, pq, pv, mq, mv, vq, vv)
    w_1, w_2, w_3 = to_all("minor", (w16,) * 3)
    own, *parts = projected_gradient(inputs, cq, cv, pq, pv)
    r_1, r_2, r_3 = to_all("major", parts)
    group, = whole_call(
        group_kernel, [jax.ShapeDtypeStruct((4 * ROWS, W), BF16)], (w16, w_1, w_2, w_3)
    )
    g_1, g_3 = shifted(group, "major", 1), shifted(group, "major", 3)
    message, = whole_call(
        partial_kernel, [jax.ShapeDtypeStruct((64, W), BF16)], (own, r_1, r_2, r_3)
    )
    m_1, m_2, m_3 = to_all("minor", (message,) * 3)
    small = lambda n: jax.ShapeDtypeStruct((16, n), F32)
    u_own, first_q, first_v, second_q, second_v = whole_call(
        update_kernel,
        [jax.ShapeDtypeStruct((64, W), BF16), small(WQ), small(WV), small(WQ), small(WV)],
        (message, m_1, m_2, m_3, w16, w_1, w_2, w_3, mq, mv, vq, vv),
        [pltpu.VMEM((64, W), F32)],
    )
    u_1, u_2, u_3 = to_all("major", (u_own,) * 3)
    h_up = shifted(g_1[: 2 * ROWS], "major", 1)
    h_down = shifted(g_3[2 * ROWS :], "major", 3)
    u, squares = whole_call(
        assemble_kernel,
        [jax.ShapeDtypeStruct((RANK, W), BF16), jax.ShapeDtypeStruct((8, 128), F32)],
        (u_own, u_1, u_2, u_3),
    )
    s_1, s_2, s_3 = to_all("x", (squares,) * 3)
    chips = (squares + s_2) + (s_1 + s_3)
    other = shifted(chips, "core", 1)
    kept = (first_q, first_v, second_q, second_v)
    new_q, new_v, step_q, step_v, copy_q, copy_v, *kept = new_weights(
        chips, other, u, pq, pv, (group, g_1, g_3, h_up, h_down), wq, wv, kept
    )
    return (new_q, new_v, copy_q, copy_v, *kept, step_q, step_v)


def solution(mesh):
    finer = Mesh(mesh.devices.reshape(SIZES), AXES)
    both, tokens, columns = P(FS, TP), P(FS, None), P(None, TP)
    return jax.shard_map(
        on_device,
        mesh=finer,
        in_specs=(tokens, both, both, P(), P()) + (both,) * 6,
        out_specs=(both, both, columns, columns) + (both,) * 6,
        check_vma=False,
    )
```

```python
import jax
import jax.numpy as jnp
from jax import lax
from jax.experimental import pallas as pl
from jax.experimental.pallas import tpu as pltpu
from jax.sharding import Mesh
from jax.sharding import PartitionSpec as P

RANK = 256
QK_W = 2048
V_W = 4096
AXES = ("z", "y", "x", "c")
SIZES = (4, 4, 4, 2)
FS = ("z", "y")
TP = ("x", "c")

beta_first = 0.9
beta_second = 0.95
adam_eps = 1e-08
norm_eps = 1e-06
step_rate = 0.05
decay_rate = 0.2

WQ = 256
WV = 512
W = WQ + WV
ROWS = 128
MESSAGE = ROWS + 32
X_BLOCKS = 3

F32 = jnp.float32
BF16 = jnp.bfloat16


def shift_pairs(kind, offset):
    pairs = []
    for z in range(4):
        for y in range(4):
            for x in range(4):
                for c in range(2):
                    to = [z, y, x, c]
                    if kind == "major":
                        axis = 0 if c == 0 else 1
                    elif kind == "minor":
                        axis = 1 if c == 0 else 0
                    elif kind == "x":
                        axis = 2
                    else:
                        axis = 3
                    to[axis] = (to[axis] + offset) % SIZES[axis]
                    source = ((z * 4 + y) * 4 + x) * 2 + c
                    target = ((to[0] * 4 + to[1]) * 4 + to[2]) * 2 + to[3]
                    pairs.append((source, target))
    return pairs


def shifted(array, kind, offset):
    return lax.ppermute(array, AXES, shift_pairs(kind, offset))


def to_all(kind, arrays):
    two = shifted(arrays[1], kind, 2)
    return shifted(arrays[0], kind, 1), two, shifted(arrays[2], kind, 3)


def own_place():
    z, y, c = lax.axis_index("z"), lax.axis_index("y"), lax.axis_index("c")
    first = c == 0
    major = jnp.where(first, z, y)
    minor = jnp.where(first, y, z)
    per_major = jnp.where(first, 4, 1)
    per_minor = jnp.where(first, 1, 4)
    return major, minor, per_major, per_minor


def in_vmem(array):
    return pltpu.with_memory_space_constraint(array, pltpu.VMEM)


def in_hbm(array):
    return pltpu.with_memory_space_constraint(array, pltpu.HBM)


def mix_kernel(
    x, cq, cv, pq, pv, wq, wv, mq, mv, vq, vv,
    mixed, w16, pq_out, pv_out, cq_out, cv_out,
    xs, wq_s, wv_s, m_s, v_s, sem, p_sem, x_sem, c_sem,
):
    half, block = mixed.shape[0], xs.shape[0] // X_BLOCKS
    core = lax.axis_index("c")
    mine = pl.multiple_of(core * half, half)
    other = pl.multiple_of((1 - core) * half, half)
    factors = [
        pltpu.make_async_copy(a, b, p_sem.at[n]) for n, (a, b) in enumerate(((pq, pq_out), (pv, pv_out)))
    ]
    blocks = [
        pltpu.make_async_copy(
            x.at[pl.ds(mine + n * block, block), :], xs.at[pl.ds(n * block, block), :], x_sem.at[n]
        )
        for n in range(X_BLOCKS)
    ]
    pairs = (
        (wq, wq_s),
        (wv, wv_s),
        (mq, m_s.at[:, pl.ds(0, WQ)]),
        (mv, m_s.at[:, pl.ds(WQ, WV)]),
        (vq, v_s.at[:, pl.ds(0, WQ)]),
        (vv, v_s.at[:, pl.ds(WQ, WV)]),
    )
    small = [pltpu.make_async_copy(a, b, sem.at[n]) for n, (a, b) in enumerate(pairs)]
    cotangents = [
        pltpu.make_async_copy(
            a.at[pl.ds(start, half), :], b.at[pl.ds(at * half, half), :], c_sem.at[n, at]
        )
        for n, (a, b) in enumerate(((cq, cq_out), (cv, cv_out)))
        for at, start in enumerate((mine, other))
    ]
    for copy in (*factors, *blocks, *small, *cotangents):
        copy.start()
    for copy in factors:
        copy.wait()
    for n in range(X_BLOCKS):
        blocks[n].wait()
        at = slice(n * block, (n + 1) * block)
        rows = xs[at, :]
        mixed[at, :RANK] = jnp.dot(rows, pq_out[...], preferred_element_type=F32).astype(BF16)
        mixed[at, RANK:] = jnp.dot(rows, pv_out[...], preferred_element_type=F32).astype(BF16)
    for copy in small:
        copy.wait()
    w16[:ROWS, :WQ] = wq_s[...].astype(BF16)
    w16[:ROWS, WQ:] = wv_s[...].astype(BF16)
    w16[ROWS : ROWS + 16, :] = m_s[...].astype(BF16)
    w16[ROWS + 16 :, :] = v_s[...].astype(BF16)
    for copy in cotangents:
        copy.wait()


def mix(inputs, cq, cv, pq, pv, *state):
    vmem, hbm = pl.BlockSpec(memory_space=pltpu.VMEM), pl.BlockSpec(memory_space=pl.ANY)
    tokens, width = inputs.shape
    half = tokens // 2
    operands = (inputs, cq, cv, pq, pv, *state)
    return pl.pallas_call(
        mix_kernel,
        in_specs=[hbm] * len(operands),
        out_specs=[vmem] * 6,
        out_shape=[
            pltpu.VMEM((half, 2 * RANK), BF16),
            pltpu.VMEM((MESSAGE, W), BF16),
            pltpu.VMEM(pq.shape, BF16),
            pltpu.VMEM(pv.shape, BF16),
            pltpu.VMEM(cq.shape, BF16),
            pltpu.VMEM(cv.shape, BF16),
        ],
        scratch_shapes=[
            pltpu.VMEM((half, width), BF16),
            pltpu.VMEM((ROWS, WQ), F32),
            pltpu.VMEM((ROWS, WV), F32),
            pltpu.VMEM((16, W), F32),
            pltpu.VMEM((16, W), F32),
            pltpu.SemaphoreType.DMA((6,)),
            pltpu.SemaphoreType.DMA((2,)),
            pltpu.SemaphoreType.DMA((X_BLOCKS,)),
            pltpu.SemaphoreType.DMA((2, 2)),
        ],
        cost_estimate=pl.CostEstimate(
            flops=4 * half * RANK * width, bytes_accessed=14_000_000, transcendentals=0
        ),
        compiler_params=pltpu.CompilerParams(vmem_limit_bytes=24 * 2**20),
        name="mix",
    )(*(in_hbm(a) for a in operands))


def lead_kernel(mixed, swapped, cq, cv, own, to_1, to_2, to_3, total):
    lead = (((0,), (0,)), ((), ()))
    half = mixed.shape[0]
    for n, held in enumerate((mixed, swapped)):
        at = slice(n * half, (n + 1) * half)
        part_q = lax.dot_general(held[:, :RANK], cq[at, :], lead, preferred_element_type=F32)
        part_v = lax.dot_general(held[:, RANK:], cv[at, :], lead, preferred_element_type=F32)
        if n == 0:
            total[:, :WQ] = part_q
            total[:, WQ:] = part_v
        else:
            total[:, :WQ] += part_q
            total[:, WQ:] += part_v
    major, _, per_major, per_minor = own_place()
    for offset, out in enumerate((own, to_1, to_2, to_3)):
        there = lax.rem(major + offset, 4)
        for minor in range(4):
            start = pl.multiple_of((there * per_major + minor * per_minor) * 16, 16)
            out[minor * 16 : (minor + 1) * 16, :] = total[pl.ds(start, 16), :].astype(out.dtype)


def whole_call(body, out, operands, scratch=(), flops=1_000_000):
    vmem = pl.BlockSpec(memory_space=pltpu.VMEM)
    return pl.pallas_call(
        body,
        in_specs=[vmem] * len(operands),
        out_specs=[vmem] * len(out),
        out_shape=[pltpu.VMEM(o.shape, o.dtype) for o in out],
        scratch_shapes=list(scratch),
        cost_estimate=pl.CostEstimate(flops=flops, bytes_accessed=1_000_000, transcendentals=0),
        compiler_params=pltpu.CompilerParams(vmem_limit_bytes=12 * 2**20),
    )(*(in_vmem(a) for a in operands))


def group_kernel(w0, w1, w2, w3, after, out):
    for n, held in enumerate((w0, w1, w2, w3)):
        out[n * ROWS : (n + 1) * ROWS, :] = held[:ROWS, :]


def partial_kernel(own, r1, r2, r3, out):
    out[...] = (own[...] + r1[...].astype(F32) + (r2[...].astype(F32) + r3[...].astype(F32))).astype(BF16)


def moments(low, first, second):
    first_new = beta_first * first + (1.0 - beta_first) * low
    second_new = beta_second * second + (1.0 - beta_second) * low * low
    return first_new, second_new


def update_kernel(own, r1, r2, r3, k0, k1, k2, k3, mq, mv, vq, vv, u, fq, fv, sq, sv, low):
    low[...] = (own[...].astype(F32) + r2[...].astype(F32)) + (r1[...].astype(F32) + r3[...].astype(F32))
    _, minor, _, _ = own_place()
    for offset, held in enumerate((k0, k1, k2, k3)):
        there = lax.rem(minor + 4 - offset, 4)
        at = pl.ds(pl.multiple_of(there * 16, 16), 16)
        first = held[ROWS : ROWS + 16, :].astype(F32)
        second = held[ROWS + 16 :, :].astype(F32)
        first, second = moments(low[at, :], first, second)
        u[at, :] = (first / (jnp.sqrt(second) + adam_eps)).astype(BF16)
    mine = low[pl.ds(pl.multiple_of(minor * 16, 16), 16), :]
    fq[...], sq[...] = moments(mine[:, :WQ], mq[...], vq[...])
    fv[...], sv[...] = moments(mine[:, WQ:], mv[...], vv[...])


def assemble_kernel(own, r1, r2, r3, u, squares):
    major, _, per_major, per_minor = own_place()
    for offset, held in enumerate((own, r1, r2, r3)):
        there = lax.rem(major + 4 - offset, 4)
        for minor in range(4):
            start = pl.multiple_of((there * per_major + minor * per_minor) * 16, 16)
            u[pl.ds(start, 16), :] = held[minor * 16 : (minor + 1) * 16, :]
    total = jnp.zeros((16, W), F32)
    for group in range(16):
        part = u[group * 16 : (group + 1) * 16, :].astype(F32)
        total += part * part
    total = total[:8, :] + total[8:, :]
    folded = total[:, :128]
    for lane in range(1, W // 128):
        folded += total[:, lane * 128 : (lane + 1) * 128]
    squares[...] = folded


def weight_kernel(
    s_own, s_other, u, pq, pv, g0, g1, g3, h_up, h_down, wq, wv, fq, fv, sq, sv,
    nq, nv, tq, tv, cq, cv, fq_out, fv_out, sq_out, sv_out,
    nq_s, nv_s, tq_s, tv_s, cq_s, cv_s, c_sem, m_sem,
):
    stores = []

    def store(source, target, sem):
        copy = pltpu.make_async_copy(source, target, sem)
        copy.start()
        stores.append(copy)

    for n, (a, b) in enumerate(((fq, fq_out), (fv, fv_out), (sq, sq_out), (sv, sv_out))):
        store(a, b, m_sem.at[n])
    major, minor, per_major, per_minor = own_place()
    squares = jnp.sum(s_own[...] + s_other[...], axis=(0, 1), keepdims=True)
    scale = lax.rsqrt(squares / (RANK * (QK_W + V_W)) + norm_eps)
    uq, uv = u[:, :WQ], u[:, WQ:]
    keep = 1.0 - step_rate * decay_rate
    for i, pieces in ((0, (g0, g0)), (1, (g1, g1)), (3, (g3, g3)), (2, (h_up, h_down))):
        a_there = lax.rem(major + 4 - i, 4)
        for j in range(4):
            b_there = lax.rem(minor + 4 - j, 4)
            block = a_there * per_major + b_there * per_minor
            at = pl.ds(pl.multiple_of(block * ROWS, ROWS), ROWS)
            back_q = scale * jnp.dot(pq[at, :], uq, preferred_element_type=F32)
            back_v = scale * jnp.dot(pv[at, :], uv, preferred_element_type=F32)
            piece = pieces[j // 2]
            top = (j if piece.shape[0] == 4 * ROWS else j % 2) * ROWS
            held = piece[top : top + ROWS, :].astype(F32)
            n = i * 4 + j
            cq_s[n] = (keep * held[:, :WQ] - step_rate * back_q).astype(BF16)
            cv_s[n] = (keep * held[:, WQ:] - step_rate * back_v).astype(BF16)
            for part, (source, target) in enumerate(((cq_s, cq), (cv_s, cv))):
                store(source.at[n], target.at[at, :], c_sem.at[n, part])
            if n == 0:
                for back, w, t, new in ((back_q, wq, tq_s, nq_s), (back_v, wv, tv_s, nv_s)):
                    weight = w[...]
                    step = back + decay_rate * weight
                    t[...] = step
                    new[...] = weight - step_rate * step
                for k, (a, b) in enumerate(((nq_s, nq), (nv_s, nv), (tq_s, tq), (tv_s, tv))):
                    store(a, b, m_sem.at[4 + k])
    for copy in stores:
        copy.wait()


def new_weights(s_own, s_other, u, pq, pv, groups, wq, wv, kept):
    vmem = pl.BlockSpec(memory_space=pltpu.VMEM)
    hbm = pl.BlockSpec(memory_space=pl.ANY)
    out = [
        jax.ShapeDtypeStruct((ROWS, WQ), F32),
        jax.ShapeDtypeStruct((ROWS, WV), F32),
        jax.ShapeDtypeStruct((ROWS, WQ), F32),
        jax.ShapeDtypeStruct((ROWS, WV), F32),
        jax.ShapeDtypeStruct((16 * ROWS, WQ), BF16),
        jax.ShapeDtypeStruct((16 * ROWS, WV), BF16),
    ] + [jax.ShapeDtypeStruct(a.shape, F32) for a in kept]
    operands = (s_own, s_other, u, pq, pv, *groups, wq, wv, *kept)
    return pl.pallas_call(
        weight_kernel,
        in_specs=[vmem] * len(operands),
        out_specs=[hbm] * len(out),
        out_shape=out,
        scratch_shapes=[
            pltpu.VMEM((ROWS, WQ), F32),
            pltpu.VMEM((ROWS, WV), F32),
            pltpu.VMEM((ROWS, WQ), F32),
            pltpu.VMEM((ROWS, WV), F32),
            pltpu.VMEM((16, ROWS, WQ), BF16),
            pltpu.VMEM((16, ROWS, WV), BF16),
            pltpu.SemaphoreType.DMA((16, 2)),
            pltpu.SemaphoreType.DMA((8,)),
        ],
        cost_estimate=pl.CostEstimate(
            flops=2 * 16 * ROWS * RANK * W, bytes_accessed=12_000_000, transcendentals=0
        ),
        compiler_params=pltpu.CompilerParams(vmem_limit_bytes=20 * 2**20),
        name="weights",
    )(*(in_vmem(a) for a in operands))


def on_device(inputs, cq, cv, pq, pv, wq, wv, mq, mv, vq, vv):
    mixed, w16, pq, pv, cq, cv = mix(inputs, cq, cv, pq, pv, wq, wv, mq, mv, vq, vv)
    swapped = shifted(mixed, "core", 1)
    w_1, w_2, w_3 = to_all("minor", (w16,) * 3)
    chunk = lambda t: jax.ShapeDtypeStruct((64, W), t)
    own, *parts = whole_call(
        lead_kernel,
        [chunk(F32), chunk(BF16), chunk(BF16), chunk(BF16)],
        (mixed, swapped, cq, cv),
        [pltpu.VMEM((RANK, W), F32)],
        flops=2 * inputs.shape[0] * RANK * W,
    )
    r_1, r_2, r_3 = to_all("major", parts)
    group, = whole_call(
        group_kernel, [jax.ShapeDtypeStruct((4 * ROWS, W), BF16)], (w16, w_1, w_2, w_3, own)
    )
    g_1, g_3 = shifted(group, "major", 1), shifted(group, "major", 3)
    message, = whole_call(
        partial_kernel, [jax.ShapeDtypeStruct((64, W), BF16)], (own, r_1, r_2, r_3)
    )
    m_1, m_2, m_3 = to_all("minor", (message,) * 3)
    small = lambda n: jax.ShapeDtypeStruct((16, n), F32)
    u_own, first_q, first_v, second_q, second_v = whole_call(
        update_kernel,
        [jax.ShapeDtypeStruct((64, W), BF16), small(WQ), small(WV), small(WQ), small(WV)],
        (message, m_1, m_2, m_3, w16, w_1, w_2, w_3, mq, mv, vq, vv),
        [pltpu.VMEM((64, W), F32)],
    )
    u_1, u_2, u_3 = to_all("major", (u_own,) * 3)
    h_up = shifted(g_1[: 2 * ROWS], "major", 1)
    h_down = shifted(g_3[2 * ROWS :], "major", 3)
    u, squares = whole_call(
        assemble_kernel,
        [jax.ShapeDtypeStruct((RANK, W), BF16), jax.ShapeDtypeStruct((8, 128), F32)],
        (u_own, u_1, u_2, u_3),
    )
    s_1, s_2, s_3 = to_all("x", (squares,) * 3)
    chips = (squares + s_2) + (s_1 + s_3)
    other = shifted(chips, "core", 1)
    kept = (first_q, first_v, second_q, second_v)
    new_q, new_v, step_q, step_v, copy_q, copy_v, *kept = new_weights(
        chips, other, u, pq, pv, (group, g_1, g_3, h_up, h_down), wq, wv, kept
    )
    return (new_q, new_v, copy_q, copy_v, *kept, step_q, step_v)


def solution(mesh):
    finer = Mesh(mesh.devices.reshape(SIZES), AXES)
    both, tokens, columns = P(FS, TP), P(FS, None), P(None, TP)
    return jax.shard_map(
        on_device,
        mesh=finer,
        in_specs=(tokens, both, both, P(), P()) + (both,) * 6,
        out_specs=(both, both, columns, columns) + (both,) * 6,
        check_vma=False,
    )
```

```python
import jax
import jax.numpy as jnp
from jax import lax
from jax.experimental import pallas as pl
from jax.experimental.pallas import tpu as pltpu
from jax.sharding import Mesh
from jax.sharding import PartitionSpec as P

RANK = 256
QK_W = 2048
V_W = 4096
AXES = ("z", "y", "x", "c")
SIZES = (4, 4, 4, 2)
FS = ("z", "y")
TP = ("x", "c")

beta_first = 0.9
beta_second = 0.95
adam_eps = 1e-08
norm_eps = 1e-06
step_rate = 0.05
decay_rate = 0.2

WQ = 256
WV = 512
W = WQ + WV
ROWS = 128
MESSAGE = ROWS + 32
X_BLOCKS = 3
DEPTHS = 4

F32 = jnp.float32
BF16 = jnp.bfloat16


def shift_pairs(kind, offset):
    pairs = []
    for z in range(4):
        for y in range(4):
            for x in range(4):
                for c in range(2):
                    to = [z, y, x, c]
                    if kind == "major":
                        axis = 0 if c == 0 else 1
                    elif kind == "minor":
                        axis = 1 if c == 0 else 0
                    elif kind == "x":
                        axis = 2
                    else:
                        axis = 3
                    to[axis] = (to[axis] + offset) % SIZES[axis]
                    source = ((z * 4 + y) * 4 + x) * 2 + c
                    target = ((to[0] * 4 + to[1]) * 4 + to[2]) * 2 + to[3]
                    pairs.append((source, target))
    return pairs


def shifted(array, kind, offset):
    return lax.ppermute(array, AXES, shift_pairs(kind, offset))


def to_all(kind, arrays):
    two = shifted(arrays[1], kind, 2)
    return shifted(arrays[0], kind, 1), two, shifted(arrays[2], kind, 3)


def own_place():
    z, y, c = lax.axis_index("z"), lax.axis_index("y"), lax.axis_index("c")
    first = c == 0
    major = jnp.where(first, z, y)
    minor = jnp.where(first, y, z)
    per_major = jnp.where(first, 4, 1)
    per_minor = jnp.where(first, 1, 4)
    return major, minor, per_major, per_minor


def in_vmem(array):
    return pltpu.with_memory_space_constraint(array, pltpu.VMEM)


def in_hbm(array):
    return pltpu.with_memory_space_constraint(array, pltpu.HBM)


def mix_kernel(
    x, cq, cv, pq, pv, wq, wv, mq, mv, vq, vv,
    mixed, w16, pq_out, pv_out, cq_out, cv_out,
    xs, wq_s, wv_s, m_s, v_s, sem, p_sem, x_sem, c_sem,
):
    half, block = mixed.shape[0], xs.shape[0] // X_BLOCKS
    core = lax.axis_index("c")
    mine = pl.multiple_of(core * half, half)
    other = pl.multiple_of((1 - core) * half, half)
    depth = pq.shape[0] // DEPTHS
    parts = [pl.ds(k * depth, depth) for k in range(DEPTHS)]
    first = [
        [
            pltpu.make_async_copy(pq.at[k, :], pq_out.at[k, :], p_sem.at[n, 0]),
            pltpu.make_async_copy(pv.at[k, :], pv_out.at[k, :], p_sem.at[n, 1]),
            pltpu.make_async_copy(x.at[pl.ds(mine, block), k], xs.at[pl.ds(0, block), k], p_sem.at[n, 2]),
        ]
        for n, k in enumerate(parts)
    ]
    blocks = [
        pltpu.make_async_copy(
            x.at[pl.ds(mine + n * block, block), :], xs.at[pl.ds(n * block, block), :], x_sem.at[n - 1]
        )
        for n in range(1, X_BLOCKS)
    ]
    pairs = (
        (wq, wq_s),
        (wv, wv_s),
        (mq, m_s.at[:, pl.ds(0, WQ)]),
        (mv, m_s.at[:, pl.ds(WQ, WV)]),
        (vq, v_s.at[:, pl.ds(0, WQ)]),
        (vv, v_s.at[:, pl.ds(WQ, WV)]),
    )
    small = [pltpu.make_async_copy(a, b, sem.at[n]) for n, (a, b) in enumerate(pairs)]
    cotangents = [
        pltpu.make_async_copy(
            a.at[pl.ds(start, half), :], b.at[pl.ds(at * half, half), :], c_sem.at[n, at]
        )
        for n, (a, b) in enumerate(((cq, cq_out), (cv, cv_out)))
        for at, start in enumerate((mine, other))
    ]
    for copy in (*(c for piece in first for c in piece), *blocks):
        copy.start()
    part_q = part_v = None
    for piece, k in zip(first, parts):
        for copy in piece:
            copy.wait()
        rows = xs[:block, k]
        piece_q = jnp.dot(rows, pq_out[k, :], preferred_element_type=F32)
        piece_v = jnp.dot(rows, pv_out[k, :], preferred_element_type=F32)
        part_q = piece_q if part_q is None else part_q + piece_q
        part_v = piece_v if part_v is None else part_v + piece_v
    for copy in (*small, *cotangents):
        copy.start()
    mixed[:block, :RANK] = part_q.astype(BF16)
    mixed[:block, RANK:] = part_v.astype(BF16)
    for n in range(1, X_BLOCKS):
        blocks[n - 1].wait()
        at = slice(n * block, (n + 1) * block)
        rows = xs[at, :]
        mixed[at, :RANK] = jnp.dot(rows, pq_out[...], preferred_element_type=F32).astype(BF16)
        mixed[at, RANK:] = jnp.dot(rows, pv_out[...], preferred_element_type=F32).astype(BF16)
    for copy in small:
        copy.wait()
    w16[:ROWS, :WQ] = wq_s[...].astype(BF16)
    w16[:ROWS, WQ:] = wv_s[...].astype(BF16)
    w16[ROWS : ROWS + 16, :] = m_s[...].astype(BF16)
    w16[ROWS + 16 :, :] = v_s[...].astype(BF16)
    for copy in cotangents:
        copy.wait()


def mix(inputs, cq, cv, pq, pv, *state):
    vmem, hbm = pl.BlockSpec(memory_space=pltpu.VMEM), pl.BlockSpec(memory_space=pl.ANY)
    tokens, width = inputs.shape
    half = tokens // 2
    operands = (inputs, cq, cv, pq, pv, *state)
    return pl.pallas_call(
        mix_kernel,
        in_specs=[hbm] * len(operands),
        out_specs=[vmem] * 6,
        out_shape=[
            pltpu.VMEM((half, 2 * RANK), BF16),
            pltpu.VMEM((MESSAGE, W), BF16),
            pltpu.VMEM(pq.shape, BF16),
            pltpu.VMEM(pv.shape, BF16),
            pltpu.VMEM(cq.shape, BF16),
            pltpu.VMEM(cv.shape, BF16),
        ],
        scratch_shapes=[
            pltpu.VMEM((half, width), BF16),
            pltpu.VMEM((ROWS, WQ), F32),
            pltpu.VMEM((ROWS, WV), F32),
            pltpu.VMEM((16, W), F32),
            pltpu.VMEM((16, W), F32),
            pltpu.SemaphoreType.DMA((6,)),
            pltpu.SemaphoreType.DMA((DEPTHS, 3)),
            pltpu.SemaphoreType.DMA((X_BLOCKS - 1,)),
            pltpu.SemaphoreType.DMA((2, 2)),
        ],
        cost_estimate=pl.CostEstimate(
            flops=4 * half * RANK * width, bytes_accessed=14_000_000, transcendentals=0
        ),
        compiler_params=pltpu.CompilerParams(vmem_limit_bytes=24 * 2**20),
        name="mix",
    )(*(in_hbm(a) for a in operands))


def lead_kernel(mixed, swapped, cq, cv, own, to_1, to_2, to_3, total):
    lead = (((0,), (0,)), ((), ()))
    half = mixed.shape[0]
    for n, held in enumerate((mixed, swapped)):
        at = slice(n * half, (n + 1) * half)
        part_q = lax.dot_general(held[:, :RANK], cq[at, :], lead, preferred_element_type=F32)
        part_v = lax.dot_general(held[:, RANK:], cv[at, :], lead, preferred_element_type=F32)
        if n == 0:
            total[:, :WQ] = part_q
            total[:, WQ:] = part_v
        else:
            total[:, :WQ] += part_q
            total[:, WQ:] += part_v
    major, _, per_major, per_minor = own_place()
    for offset, out in enumerate((own, to_1, to_2, to_3)):
        there = lax.rem(major + offset, 4)
        for minor in range(4):
            start = pl.multiple_of((there * per_major + minor * per_minor) * 16, 16)
            out[minor * 16 : (minor + 1) * 16, :] = total[pl.ds(start, 16), :].astype(out.dtype)


def whole_call(body, out, operands, scratch=(), flops=1_000_000):
    vmem = pl.BlockSpec(memory_space=pltpu.VMEM)
    return pl.pallas_call(
        body,
        in_specs=[vmem] * len(operands),
        out_specs=[vmem] * len(out),
        out_shape=[pltpu.VMEM(o.shape, o.dtype) for o in out],
        scratch_shapes=list(scratch),
        cost_estimate=pl.CostEstimate(flops=flops, bytes_accessed=1_000_000, transcendentals=0),
        compiler_params=pltpu.CompilerParams(vmem_limit_bytes=12 * 2**20),
    )(*(in_vmem(a) for a in operands))


def group_kernel(w0, w1, w2, w3, after, out):
    for n, held in enumerate((w0, w1, w2, w3)):
        out[n * ROWS : (n + 1) * ROWS, :] = held[:ROWS, :]


def partial_kernel(own, r1, r2, r3, out):
    out[...] = (own[...] + r1[...].astype(F32) + (r2[...].astype(F32) + r3[...].astype(F32))).astype(BF16)


def moments(low, first, second):
    first_new = beta_first * first + (1.0 - beta_first) * low
    second_new = beta_second * second + (1.0 - beta_second) * low * low
    return first_new, second_new


def update_kernel(own, r1, r2, r3, k0, k1, k2, k3, mq, mv, vq, vv, u, fq, fv, sq, sv, low):
    low[...] = (own[...].astype(F32) + r2[...].astype(F32)) + (r1[...].astype(F32) + r3[...].astype(F32))
    _, minor, _, _ = own_place()
    for offset, held in enumerate((k0, k1, k2, k3)):
        there = lax.rem(minor + 4 - offset, 4)
        at = pl.ds(pl.multiple_of(there * 16, 16), 16)
        first = held[ROWS : ROWS + 16, :].astype(F32)
        second = held[ROWS + 16 :, :].astype(F32)
        first, second = moments(low[at, :], first, second)
        u[at, :] = (first / (jnp.sqrt(second) + adam_eps)).astype(BF16)
    mine = low[pl.ds(pl.multiple_of(minor * 16, 16), 16), :]
    fq[...], sq[...] = moments(mine[:, :WQ], mq[...], vq[...])
    fv[...], sv[...] = moments(mine[:, WQ:], mv[...], vv[...])


def assemble_kernel(own, r1, r2, r3, u, squares):
    major, _, per_major, per_minor = own_place()
    for offset, held in enumerate((own, r1, r2, r3)):
        there = lax.rem(major + 4 - offset, 4)
        for minor in range(4):
            start = pl.multiple_of((there * per_major + minor * per_minor) * 16, 16)
            u[pl.ds(start, 16), :] = held[minor * 16 : (minor + 1) * 16, :]
    total = jnp.zeros((16, W), F32)
    for group in range(16):
        part = u[group * 16 : (group + 1) * 16, :].astype(F32)
        total += part * part
    total = total[:8, :] + total[8:, :]
    folded = total[:, :128]
    for lane in range(1, W // 128):
        folded += total[:, lane * 128 : (lane + 1) * 128]
    squares[...] = folded


def weight_kernel(
    s_own, s_other, u, pq, pv, g0, g1, g3, h_up, h_down, wq, wv, fq, fv, sq, sv,
    nq, nv, tq, tv, cq, cv, fq_out, fv_out, sq_out, sv_out,
    nq_s, nv_s, tq_s, tv_s, cq_s, cv_s, c_sem, m_sem,
):
    stores = []

    def store(source, target, sem):
        copy = pltpu.make_async_copy(source, target, sem)
        copy.start()
        stores.append(copy)

    for n, (a, b) in enumerate(((fq, fq_out), (fv, fv_out), (sq, sq_out), (sv, sv_out))):
        store(a, b, m_sem.at[n])
    major, minor, per_major, per_minor = own_place()
    squares = jnp.sum(s_own[...] + s_other[...], axis=(0, 1), keepdims=True)
    scale = lax.rsqrt(squares / (RANK * (QK_W + V_W)) + norm_eps)
    uq, uv = u[:, :WQ], u[:, WQ:]
    keep = 1.0 - step_rate * decay_rate
    for i, pieces in ((0, (g0, g0)), (1, (g1, g1)), (3, (g3, g3)), (2, (h_up, h_down))):
        a_there = lax.rem(major + 4 - i, 4)
        for j in range(4):
            b_there = lax.rem(minor + 4 - j, 4)
            block = a_there * per_major + b_there * per_minor
            at = pl.ds(pl.multiple_of(block * ROWS, ROWS), ROWS)
            back_q = scale * jnp.dot(pq[at, :], uq, preferred_element_type=F32)
            back_v = scale * jnp.dot(pv[at, :], uv, preferred_element_type=F32)
            piece = pieces[j // 2]
            top = (j if piece.shape[0] == 4 * ROWS else j % 2) * ROWS
            held = piece[top : top + ROWS, :].astype(F32)
            n = i * 4 + j
            cq_s[n] = (keep * held[:, :WQ] - step_rate * back_q).astype(BF16)
            cv_s[n] = (keep * held[:, WQ:] - step_rate * back_v).astype(BF16)
            for part, (source, target) in enumerate(((cq_s, cq), (cv_s, cv))):
                store(source.at[n], target.at[at, :], c_sem.at[n, part])
            if n == 0:
                for back, w, t, new in ((back_q, wq, tq_s, nq_s), (back_v, wv, tv_s, nv_s)):
                    weight = w[...]
                    step = back + decay_rate * weight
                    t[...] = step
                    new[...] = weight - step_rate * step
                for k, (a, b) in enumerate(((nq_s, nq), (nv_s, nv), (tq_s, tq), (tv_s, tv))):
                    store(a, b, m_sem.at[4 + k])
    for copy in stores:
        copy.wait()


def new_weights(s_own, s_other, u, pq, pv, groups, wq, wv, kept):
    vmem = pl.BlockSpec(memory_space=pltpu.VMEM)
    hbm = pl.BlockSpec(memory_space=pl.ANY)
    out = [
        jax.ShapeDtypeStruct((ROWS, WQ), F32),
        jax.ShapeDtypeStruct((ROWS, WV), F32),
        jax.ShapeDtypeStruct((ROWS, WQ), F32),
        jax.ShapeDtypeStruct((ROWS, WV), F32),
        jax.ShapeDtypeStruct((16 * ROWS, WQ), BF16),
        jax.ShapeDtypeStruct((16 * ROWS, WV), BF16),
    ] + [jax.ShapeDtypeStruct(a.shape, F32) for a in kept]
    operands = (s_own, s_other, u, pq, pv, *groups, wq, wv, *kept)
    return pl.pallas_call(
        weight_kernel,
        in_specs=[vmem] * len(operands),
        out_specs=[hbm] * len(out),
        out_shape=out,
        scratch_shapes=[
            pltpu.VMEM((ROWS, WQ), F32),
            pltpu.VMEM((ROWS, WV), F32),
            pltpu.VMEM((ROWS, WQ), F32),
            pltpu.VMEM((ROWS, WV), F32),
            pltpu.VMEM((16, ROWS, WQ), BF16),
            pltpu.VMEM((16, ROWS, WV), BF16),
            pltpu.SemaphoreType.DMA((16, 2)),
            pltpu.SemaphoreType.DMA((8,)),
        ],
        cost_estimate=pl.CostEstimate(
            flops=2 * 16 * ROWS * RANK * W, bytes_accessed=12_000_000, transcendentals=0
        ),
        compiler_params=pltpu.CompilerParams(vmem_limit_bytes=20 * 2**20),
        name="weights",
    )(*(in_vmem(a) for a in operands))


def on_device(inputs, cq, cv, pq, pv, wq, wv, mq, mv, vq, vv):
    mixed, w16, pq, pv, cq, cv = mix(inputs, cq, cv, pq, pv, wq, wv, mq, mv, vq, vv)
    swapped = shifted(mixed, "core", 1)
    w_1, w_2, w_3 = to_all("minor", (w16,) * 3)
    chunk = lambda t: jax.ShapeDtypeStruct((64, W), t)
    own, *parts = whole_call(
        lead_kernel,
        [chunk(F32), chunk(BF16), chunk(BF16), chunk(BF16)],
        (mixed, swapped, cq, cv),
        [pltpu.VMEM((RANK, W), F32)],
        flops=2 * inputs.shape[0] * RANK * W,
    )
    r_1, r_2, r_3 = to_all("major", parts)
    group, = whole_call(
        group_kernel, [jax.ShapeDtypeStruct((4 * ROWS, W), BF16)], (w16, w_1, w_2, w_3, own)
    )
    g_1, g_3 = shifted(group, "major", 1), shifted(group, "major", 3)
    message, = whole_call(
        partial_kernel, [jax.ShapeDtypeStruct((64, W), BF16)], (own, r_1, r_2, r_3)
    )
    m_1, m_2, m_3 = to_all("minor", (message,) * 3)
    small = lambda n: jax.ShapeDtypeStruct((16, n), F32)
    u_own, first_q, first_v, second_q, second_v = whole_call(
        update_kernel,
        [jax.ShapeDtypeStruct((64, W), BF16), small(WQ), small(WV), small(WQ), small(WV)],
        (message, m_1, m_2, m_3, w16, w_1, w_2, w_3, mq, mv, vq, vv),
        [pltpu.VMEM((64, W), F32)],
    )
    u_1, u_2, u_3 = to_all("major", (u_own,) * 3)
    h_up = shifted(g_1[: 2 * ROWS], "major", 1)
    h_down = shifted(g_3[2 * ROWS :], "major", 3)
    u, squares = whole_call(
        assemble_kernel,
        [jax.ShapeDtypeStruct((RANK, W), BF16), jax.ShapeDtypeStruct((8, 128), F32)],
        (u_own, u_1, u_2, u_3),
    )
    s_1, s_2, s_3 = to_all("x", (squares,) * 3)
    chips = (squares + s_2) + (s_1 + s_3)
    other = shifted(chips, "core", 1)
    kept = (first_q, first_v, second_q, second_v)
    new_q, new_v, step_q, step_v, copy_q, copy_v, *kept = new_weights(
        chips, other, u, pq, pv, (group, g_1, g_3, h_up, h_down), wq, wv, kept
    )
    return (new_q, new_v, copy_q, copy_v, *kept, step_q, step_v)


def solution(mesh):
    finer = Mesh(mesh.devices.reshape(SIZES), AXES)
    both, tokens, columns = P(FS, TP), P(FS, None), P(None, TP)
    return jax.shard_map(
        on_device,
        mesh=finer,
        in_specs=(tokens, both, both, P(), P()) + (both,) * 6,
        out_specs=(both, both, columns, columns) + (both,) * 6,
        check_vma=False,
    )
```

```python
import jax
import jax.numpy as jnp
from jax import lax
from jax.experimental import pallas as pl
from jax.experimental.pallas import tpu as pltpu
from jax.sharding import Mesh
from jax.sharding import PartitionSpec as P

RANK = 256
QK_W = 2048
V_W = 4096
AXES = ("z", "y", "x", "c")
SIZES = (4, 4, 4, 2)
FS = ("z", "y")
TP = ("x", "c")

beta_first = 0.9
beta_second = 0.95
adam_eps = 1e-08
norm_eps = 1e-06
step_rate = 0.05
decay_rate = 0.2

WQ = 256
WV = 512
W = WQ + WV
ROWS = 128
MESSAGE = ROWS + 32
X_BLOCKS = 3
DEPTHS = 4

F32 = jnp.float32
BF16 = jnp.bfloat16


def shift_pairs(kind, offset):
    pairs = []
    for z in range(4):
        for y in range(4):
            for x in range(4):
                for c in range(2):
                    to = [z, y, x, c]
                    if kind == "major":
                        axis = 0 if c == 0 else 1
                    elif kind == "minor":
                        axis = 1 if c == 0 else 0
                    elif kind == "x":
                        axis = 2
                    else:
                        axis = 3
                    to[axis] = (to[axis] + offset) % SIZES[axis]
                    source = ((z * 4 + y) * 4 + x) * 2 + c
                    target = ((to[0] * 4 + to[1]) * 4 + to[2]) * 2 + to[3]
                    pairs.append((source, target))
    return pairs


def shifted(array, kind, offset):
    return lax.ppermute(array, AXES, shift_pairs(kind, offset))


def to_all(kind, arrays):
    two = shifted(arrays[1], kind, 2)
    return shifted(arrays[0], kind, 1), two, shifted(arrays[2], kind, 3)


def own_place():
    z, y, c = lax.axis_index("z"), lax.axis_index("y"), lax.axis_index("c")
    first = c == 0
    major = jnp.where(first, z, y)
    minor = jnp.where(first, y, z)
    per_major = jnp.where(first, 4, 1)
    per_minor = jnp.where(first, 1, 4)
    return major, minor, per_major, per_minor


def in_vmem(array):
    return pltpu.with_memory_space_constraint(array, pltpu.VMEM)


def in_hbm(array):
    return pltpu.with_memory_space_constraint(array, pltpu.HBM)


def mix_kernel(
    x, cq, cv, pq, pv, wq, wv, mq, mv, vq, vv,
    mixed, w16, pq_out, pv_out, cq_out, cv_out,
    xs, wq_s, wv_s, m_s, v_s, sem, p_sem, x_sem, c_sem,
):
    half, block = mixed.shape[0], xs.shape[0] // X_BLOCKS
    core = lax.axis_index("c")
    mine = pl.multiple_of(core * half, half)
    other = pl.multiple_of((1 - core) * half, half)
    depth = pq.shape[0] // DEPTHS
    parts = [pl.ds(k * depth, depth) for k in range(DEPTHS)]
    first = [
        [
            pltpu.make_async_copy(pq.at[k, :], pq_out.at[k, :], p_sem.at[n, 0]),
            pltpu.make_async_copy(pv.at[k, :], pv_out.at[k, :], p_sem.at[n, 1]),
            pltpu.make_async_copy(x.at[pl.ds(mine, block), k], xs.at[pl.ds(0, block), k], p_sem.at[n, 2]),
        ]
        for n, k in enumerate(parts)
    ]
    blocks = [
        pltpu.make_async_copy(
            x.at[pl.ds(mine + n * block, block), :], xs.at[pl.ds(n * block, block), :], x_sem.at[n - 1]
        )
        for n in range(1, X_BLOCKS)
    ]
    pairs = (
        (wq, wq_s),
        (wv, wv_s),
        (mq, m_s.at[:, pl.ds(0, WQ)]),
        (mv, m_s.at[:, pl.ds(WQ, WV)]),
        (vq, v_s.at[:, pl.ds(0, WQ)]),
        (vv, v_s.at[:, pl.ds(WQ, WV)]),
    )
    small = [pltpu.make_async_copy(a, b, sem.at[n]) for n, (a, b) in enumerate(pairs)]
    cotangents = [
        pltpu.make_async_copy(
            a.at[pl.ds(start, half), :], b.at[pl.ds(at * half, half), :], c_sem.at[n, at]
        )
        for n, (a, b) in enumerate(((cq, cq_out), (cv, cv_out)))
        for at, start in enumerate((mine, other))
    ]
    for copy in (*(c for piece in first for c in piece), *blocks):
        copy.start()
    part_q = part_v = None
    for piece, k in zip(first, parts):
        for copy in piece:
            copy.wait()
        rows = xs[:block, k]
        piece_q = jnp.dot(rows, pq_out[k, :], preferred_element_type=F32)
        piece_v = jnp.dot(rows, pv_out[k, :], preferred_element_type=F32)
        part_q = piece_q if part_q is None else part_q + piece_q
        part_v = piece_v if part_v is None else part_v + piece_v
    for copy in (*small, *cotangents):
        copy.start()
    mixed[:block, :RANK] = part_q.astype(BF16)
    mixed[:block, RANK:] = part_v.astype(BF16)
    for n in range(1, X_BLOCKS):
        blocks[n - 1].wait()
        at = slice(n * block, (n + 1) * block)
        rows = xs[at, :]
        mixed[at, :RANK] = jnp.dot(rows, pq_out[...], preferred_element_type=F32).astype(BF16)
        mixed[at, RANK:] = jnp.dot(rows, pv_out[...], preferred_element_type=F32).astype(BF16)
    for copy in small:
        copy.wait()
    w16[:ROWS, :WQ] = wq_s[...].astype(BF16)
    w16[:ROWS, WQ:] = wv_s[...].astype(BF16)
    w16[ROWS : ROWS + 16, :] = m_s[...].astype(BF16)
    w16[ROWS + 16 :, :] = v_s[...].astype(BF16)
    for copy in cotangents:
        copy.wait()


def mix(inputs, cq, cv, pq, pv, *state):
    vmem, hbm = pl.BlockSpec(memory_space=pltpu.VMEM), pl.BlockSpec(memory_space=pl.ANY)
    tokens, width = inputs.shape
    half = tokens // 2
    operands = (inputs, cq, cv, pq, pv, *state)
    return pl.pallas_call(
        mix_kernel,
        in_specs=[hbm] * len(operands),
        out_specs=[vmem] * 6,
        out_shape=[
            pltpu.VMEM((half, 2 * RANK), BF16),
            pltpu.VMEM((MESSAGE, W), BF16),
            pltpu.VMEM(pq.shape, BF16),
            pltpu.VMEM(pv.shape, BF16),
            pltpu.VMEM(cq.shape, BF16),
            pltpu.VMEM(cv.shape, BF16),
        ],
        scratch_shapes=[
            pltpu.VMEM((half, width), BF16),
            pltpu.VMEM((ROWS, WQ), F32),
            pltpu.VMEM((ROWS, WV), F32),
            pltpu.VMEM((16, W), F32),
            pltpu.VMEM((16, W), F32),
            pltpu.SemaphoreType.DMA((6,)),
            pltpu.SemaphoreType.DMA((DEPTHS, 3)),
            pltpu.SemaphoreType.DMA((X_BLOCKS - 1,)),
            pltpu.SemaphoreType.DMA((2, 2)),
        ],
        cost_estimate=pl.CostEstimate(
            flops=4 * half * RANK * width, bytes_accessed=14_000_000, transcendentals=0
        ),
        compiler_params=pltpu.CompilerParams(vmem_limit_bytes=24 * 2**20),
        name="mix",
    )(*(in_hbm(a) for a in operands))


def lead_kernel(mixed, swapped, cq, cv, own, to_1, to_2, to_3, total):
    lead = (((0,), (0,)), ((), ()))
    half = mixed.shape[0]
    for n, held in enumerate((mixed, swapped)):
        at = slice(n * half, (n + 1) * half)
        part_q = lax.dot_general(held[:, :RANK], cq[at, :], lead, preferred_element_type=F32)
        part_v = lax.dot_general(held[:, RANK:], cv[at, :], lead, preferred_element_type=F32)
        if n == 0:
            total[:, :WQ] = part_q
            total[:, WQ:] = part_v
        else:
            total[:, :WQ] += part_q
            total[:, WQ:] += part_v
    major, _, per_major, per_minor = own_place()
    for offset, out in enumerate((own, to_1, to_2, to_3)):
        there = lax.rem(major + offset, 4)
        for minor in range(4):
            start = pl.multiple_of((there * per_major + minor * per_minor) * 16, 16)
            out[minor * 16 : (minor + 1) * 16, :] = total[pl.ds(start, 16), :].astype(out.dtype)


def whole_call(body, out, operands, scratch=(), flops=1_000_000):
    vmem = pl.BlockSpec(memory_space=pltpu.VMEM)
    return pl.pallas_call(
        body,
        in_specs=[vmem] * len(operands),
        out_specs=[vmem] * len(out),
        out_shape=[pltpu.VMEM(o.shape, o.dtype) for o in out],
        scratch_shapes=list(scratch),
        cost_estimate=pl.CostEstimate(flops=flops, bytes_accessed=1_000_000, transcendentals=0),
        compiler_params=pltpu.CompilerParams(vmem_limit_bytes=12 * 2**20),
    )(*(in_vmem(a) for a in operands))


def group_kernel(w0, w1, w2, w3, after, out):
    for n, held in enumerate((w0, w1, w2, w3)):
        out[n * ROWS : (n + 1) * ROWS, :] = held[:ROWS, :]


def partial_kernel(own, r1, r2, r3, out):
    out[...] = (own[...] + r1[...].astype(F32) + (r2[...].astype(F32) + r3[...].astype(F32))).astype(BF16)


def moments(low, first, second):
    first_new = beta_first * first + (1.0 - beta_first) * low
    second_new = beta_second * second + (1.0 - beta_second) * low * low
    return first_new, second_new


def update_kernel(own, r1, r2, r3, k0, k1, k2, k3, mq, mv, vq, vv, u, fq, fv, sq, sv, low):
    low[...] = (own[...].astype(F32) + r2[...].astype(F32)) + (r1[...].astype(F32) + r3[...].astype(F32))
    _, minor, _, _ = own_place()
    for offset, held in enumerate((k0, k1, k2, k3)):
        there = lax.rem(minor + 4 - offset, 4)
        at = pl.ds(pl.multiple_of(there * 16, 16), 16)
        first = held[ROWS : ROWS + 16, :].astype(F32)
        second = held[ROWS + 16 :, :].astype(F32)
        first, second = moments(low[at, :], first, second)
        u[at, :] = (first / (jnp.sqrt(second) + adam_eps)).astype(BF16)
    mine = low[pl.ds(pl.multiple_of(minor * 16, 16), 16), :]
    fq[...], sq[...] = moments(mine[:, :WQ], mq[...], vq[...])
    fv[...], sv[...] = moments(mine[:, WQ:], mv[...], vv[...])


def assemble_kernel(own, r1, r2, r3, u, squares):
    major, _, per_major, per_minor = own_place()
    for offset, held in enumerate((own, r1, r2, r3)):
        there = lax.rem(major + 4 - offset, 4)
        for minor in range(4):
            start = pl.multiple_of((there * per_major + minor * per_minor) * 16, 16)
            u[pl.ds(start, 16), :] = held[minor * 16 : (minor + 1) * 16, :]
    total = jnp.zeros((16, W), F32)
    for group in range(16):
        part = u[group * 16 : (group + 1) * 16, :].astype(F32)
        total += part * part
    total = total[:8, :] + total[8:, :]
    folded = total[:, :128]
    for lane in range(1, W // 128):
        folded += total[:, lane * 128 : (lane + 1) * 128]
    squares[...] = folded


def weight_kernel(
    s_own, s_other, u, pq, pv, g0, g1, g2, g3, wq, wv, fq, fv, sq, sv,
    nq, nv, tq, tv, cq, cv, fq_out, fv_out, sq_out, sv_out,
    nq_s, nv_s, tq_s, tv_s, cq_s, cv_s, c_sem, m_sem,
):
    stores = []

    def store(source, target, sem):
        copy = pltpu.make_async_copy(source, target, sem)
        copy.start()
        stores.append(copy)

    for n, (a, b) in enumerate(((fq, fq_out), (fv, fv_out), (sq, sq_out), (sv, sv_out))):
        store(a, b, m_sem.at[n])
    major, minor, per_major, per_minor = own_place()
    squares = jnp.sum(s_own[...] + s_other[...], axis=(0, 1), keepdims=True)
    scale = lax.rsqrt(squares / (RANK * (QK_W + V_W)) + norm_eps)
    uq, uv = u[:, :WQ], u[:, WQ:]
    keep = 1.0 - step_rate * decay_rate
    for i, piece in ((0, g0), (1, g1), (3, g3), (2, g2)):
        a_there = lax.rem(major + 4 - i, 4)
        for j in range(4):
            b_there = lax.rem(minor + 4 - j, 4)
            block = a_there * per_major + b_there * per_minor
            at = pl.ds(pl.multiple_of(block * ROWS, ROWS), ROWS)
            back_q = scale * jnp.dot(pq[at, :], uq, preferred_element_type=F32)
            back_v = scale * jnp.dot(pv[at, :], uv, preferred_element_type=F32)
            held = piece[j * ROWS : (j + 1) * ROWS, :].astype(F32)
            n = i * 4 + j
            cq_s[n] = (keep * held[:, :WQ] - step_rate * back_q).astype(BF16)
            cv_s[n] = (keep * held[:, WQ:] - step_rate * back_v).astype(BF16)
            for part, (source, target) in enumerate(((cq_s, cq), (cv_s, cv))):
                store(source.at[n], target.at[at, :], c_sem.at[n, part])
            if n == 0:
                for back, w, t, new in ((back_q, wq, tq_s, nq_s), (back_v, wv, tv_s, nv_s)):
                    weight = w[...]
                    step = back + decay_rate * weight
                    t[...] = step
                    new[...] = weight - step_rate * step
                for k, (a, b) in enumerate(((nq_s, nq), (nv_s, nv), (tq_s, tq), (tv_s, tv))):
                    store(a, b, m_sem.at[4 + k])
    for copy in stores:
        copy.wait()


def new_weights(s_own, s_other, u, pq, pv, groups, wq, wv, kept):
    vmem = pl.BlockSpec(memory_space=pltpu.VMEM)
    hbm = pl.BlockSpec(memory_space=pl.ANY)
    out = [
        jax.ShapeDtypeStruct((ROWS, WQ), F32),
        jax.ShapeDtypeStruct((ROWS, WV), F32),
        jax.ShapeDtypeStruct((ROWS, WQ), F32),
        jax.ShapeDtypeStruct((ROWS, WV), F32),
        jax.ShapeDtypeStruct((16 * ROWS, WQ), BF16),
        jax.ShapeDtypeStruct((16 * ROWS, WV), BF16),
    ] + [jax.ShapeDtypeStruct(a.shape, F32) for a in kept]
    operands = (s_own, s_other, u, pq, pv, *groups, wq, wv, *kept)
    return pl.pallas_call(
        weight_kernel,
        in_specs=[vmem] * len(operands),
        out_specs=[hbm] * len(out),
        out_shape=out,
        scratch_shapes=[
            pltpu.VMEM((ROWS, WQ), F32),
            pltpu.VMEM((ROWS, WV), F32),
            pltpu.VMEM((ROWS, WQ), F32),
            pltpu.VMEM((ROWS, WV), F32),
            pltpu.VMEM((16, ROWS, WQ), BF16),
            pltpu.VMEM((16, ROWS, WV), BF16),
            pltpu.SemaphoreType.DMA((16, 2)),
            pltpu.SemaphoreType.DMA((8,)),
        ],
        cost_estimate=pl.CostEstimate(
            flops=2 * 16 * ROWS * RANK * W, bytes_accessed=12_000_000, transcendentals=0
        ),
        compiler_params=pltpu.CompilerParams(vmem_limit_bytes=20 * 2**20),
        name="weights",
    )(*(in_vmem(a) for a in operands))


def on_device(inputs, cq, cv, pq, pv, wq, wv, mq, mv, vq, vv):
    mixed, w16, pq, pv, cq, cv = mix(inputs, cq, cv, pq, pv, wq, wv, mq, mv, vq, vv)
    swapped = shifted(mixed, "core", 1)
    w_1, w_2, w_3 = to_all("minor", (w16,) * 3)
    chunk = lambda t: jax.ShapeDtypeStruct((64, W), t)
    own, *parts = whole_call(
        lead_kernel,
        [chunk(F32), chunk(BF16), chunk(BF16), chunk(BF16)],
        (mixed, swapped, cq, cv),
        [pltpu.VMEM((RANK, W), F32)],
        flops=2 * inputs.shape[0] * RANK * W,
    )
    r_1, r_2, r_3 = to_all("major", parts)
    group, = whole_call(
        group_kernel, [jax.ShapeDtypeStruct((4 * ROWS, W), BF16)], (w16, w_1, w_2, w_3, own)
    )
    g_1, g_3 = shifted(group, "major", 1), shifted(group, "major", 3)
    message, = whole_call(
        partial_kernel, [jax.ShapeDtypeStruct((64, W), BF16)], (own, r_1, r_2, r_3)
    )
    m_1, m_2, m_3 = to_all("minor", (message,) * 3)
    small = lambda n: jax.ShapeDtypeStruct((16, n), F32)
    u_own, first_q, first_v, second_q, second_v = whole_call(
        update_kernel,
        [jax.ShapeDtypeStruct((64, W), BF16), small(WQ), small(WV), small(WQ), small(WV)],
        (message, m_1, m_2, m_3, w16, w_1, w_2, w_3, mq, mv, vq, vv),
        [pltpu.VMEM((64, W), F32)],
    )
    u_1, u_2, u_3 = to_all("major", (u_own,) * 3)
    g_2 = shifted(g_3, "major", 3)
    u, squares = whole_call(
        assemble_kernel,
        [jax.ShapeDtypeStruct((RANK, W), BF16), jax.ShapeDtypeStruct((8, 128), F32)],
        (u_own, u_1, u_2, u_3),
    )
    s_1, s_2, s_3 = to_all("x", (squares,) * 3)
    chips = (squares + s_2) + (s_1 + s_3)
    other = shifted(chips, "core", 1)
    kept = (first_q, first_v, second_q, second_v)
    new_q, new_v, step_q, step_v, copy_q, copy_v, *kept = new_weights(
        chips, other, u, pq, pv, (group, g_1, g_2, g_3), wq, wv, kept
    )
    return (new_q, new_v, copy_q, copy_v, *kept, step_q, step_v)


def solution(mesh):
    finer = Mesh(mesh.devices.reshape(SIZES), AXES)
    both, tokens, columns = P(FS, TP), P(FS, None), P(None, TP)
    return jax.shard_map(
        on_device,
        mesh=finer,
        in_specs=(tokens, both, both, P(), P()) + (both,) * 6,
        out_specs=(both, both, columns, columns) + (both,) * 6,
        check_vma=False,
    )
```

```python
import jax
import jax.numpy as jnp
from jax import lax
from jax.experimental import pallas as pl
from jax.experimental.pallas import tpu as pltpu
from jax.sharding import Mesh
from jax.sharding import PartitionSpec as P

RANK = 256
QK_W = 2048
V_W = 4096
AXES = ("z", "y", "x", "c")
SIZES = (4, 4, 4, 2)
FS = ("z", "y")
TP = ("x", "c")

beta_first = 0.9
beta_second = 0.95
adam_eps = 1e-08
norm_eps = 1e-06
step_rate = 0.05
decay_rate = 0.2

WQ = 256
WV = 512
W = WQ + WV
ROWS = 128
MESSAGE = ROWS + 32
X_BLOCKS = 3
DEPTHS = 4

F32 = jnp.float32
BF16 = jnp.bfloat16


def shift_pairs(kind, offset):
    pairs = []
    for z in range(4):
        for y in range(4):
            for x in range(4):
                for c in range(2):
                    to = [z, y, x, c]
                    if kind == "major":
                        axis = 0 if c == 0 else 1
                    elif kind == "minor":
                        axis = 1 if c == 0 else 0
                    elif kind == "x":
                        axis = 2
                    else:
                        axis = 3
                    to[axis] = (to[axis] + offset) % SIZES[axis]
                    source = ((z * 4 + y) * 4 + x) * 2 + c
                    target = ((to[0] * 4 + to[1]) * 4 + to[2]) * 2 + to[3]
                    pairs.append((source, target))
    return pairs


def shifted(array, kind, offset):
    return lax.ppermute(array, AXES, shift_pairs(kind, offset))


def to_all(kind, arrays):
    two = shifted(arrays[1], kind, 2)
    return shifted(arrays[0], kind, 1), two, shifted(arrays[2], kind, 3)


def own_place():
    z, y, c = lax.axis_index("z"), lax.axis_index("y"), lax.axis_index("c")
    first = c == 0
    major = jnp.where(first, z, y)
    minor = jnp.where(first, y, z)
    per_major = jnp.where(first, 4, 1)
    per_minor = jnp.where(first, 1, 4)
    return major, minor, per_major, per_minor


def in_vmem(array):
    return pltpu.with_memory_space_constraint(array, pltpu.VMEM)


def in_hbm(array):
    return pltpu.with_memory_space_constraint(array, pltpu.HBM)


def mix_kernel(
    x, cq, cv, pq, pv, wq, wv, mq, mv, vq, vv,
    mixed, w16, pq_out, pv_out, cq_out, cv_out,
    xs, wq_s, wv_s, m_s, v_s, sem, p_sem, x_sem, c_sem,
):
    half, block = mixed.shape[0], xs.shape[0] // X_BLOCKS
    core = lax.axis_index("c")
    mine = pl.multiple_of(core * half, half)
    other = pl.multiple_of((1 - core) * half, half)
    depth = pq.shape[0] // DEPTHS
    parts = [pl.ds(k * depth, depth) for k in range(DEPTHS)]
    first = [
        [
            pltpu.make_async_copy(pq.at[k, :], pq_out.at[k, :], p_sem.at[n, 0]),
            pltpu.make_async_copy(pv.at[k, :], pv_out.at[k, :], p_sem.at[n, 1]),
            pltpu.make_async_copy(x.at[pl.ds(mine, block), k], xs.at[pl.ds(0, block), k], p_sem.at[n, 2]),
        ]
        for n, k in enumerate(parts)
    ]
    blocks = [
        pltpu.make_async_copy(
            x.at[pl.ds(mine + n * block, block), :], xs.at[pl.ds(n * block, block), :], x_sem.at[n - 1]
        )
        for n in range(1, X_BLOCKS)
    ]
    pairs = (
        (wq, wq_s),
        (wv, wv_s),
        (mq, m_s.at[:, pl.ds(0, WQ)]),
        (mv, m_s.at[:, pl.ds(WQ, WV)]),
        (vq, v_s.at[:, pl.ds(0, WQ)]),
        (vv, v_s.at[:, pl.ds(WQ, WV)]),
    )
    small = [pltpu.make_async_copy(a, b, sem.at[n]) for n, (a, b) in enumerate(pairs)]
    cotangents = [
        pltpu.make_async_copy(
            a.at[pl.ds(start, half), :], b.at[pl.ds(at * half, half), :], c_sem.at[n, at]
        )
        for n, (a, b) in enumerate(((cq, cq_out), (cv, cv_out)))
        for at, start in enumerate((mine, other))
    ]
    for copy in (*(c for piece in first for c in piece), *blocks):
        copy.start()
    part_q = part_v = None
    for piece, k in zip(first, parts):
        for copy in piece:
            copy.wait()
        rows = xs[:block, k]
        piece_q = jnp.dot(rows, pq_out[k, :], preferred_element_type=F32)
        piece_v = jnp.dot(rows, pv_out[k, :], preferred_element_type=F32)
        part_q = piece_q if part_q is None else part_q + piece_q
        part_v = piece_v if part_v is None else part_v + piece_v
    for copy in (*small, *cotangents):
        copy.start()
    mixed[:block, :RANK] = part_q.astype(BF16)
    mixed[:block, RANK:] = part_v.astype(BF16)
    for n in range(1, X_BLOCKS):
        blocks[n - 1].wait()
        at = slice(n * block, (n + 1) * block)
        rows = xs[at, :]
        mixed[at, :RANK] = jnp.dot(rows, pq_out[...], preferred_element_type=F32).astype(BF16)
        mixed[at, RANK:] = jnp.dot(rows, pv_out[...], preferred_element_type=F32).astype(BF16)
    for copy in small:
        copy.wait()
    w16[:ROWS, :WQ] = wq_s[...].astype(BF16)
    w16[:ROWS, WQ:] = wv_s[...].astype(BF16)
    w16[ROWS : ROWS + 16, :] = m_s[...].astype(BF16)
    w16[ROWS + 16 :, :] = v_s[...].astype(BF16)
    for copy in cotangents:
        copy.wait()


def mix(inputs, cq, cv, pq, pv, *state):
    vmem, hbm = pl.BlockSpec(memory_space=pltpu.VMEM), pl.BlockSpec(memory_space=pl.ANY)
    tokens, width = inputs.shape
    half = tokens // 2
    operands = (inputs, cq, cv, pq, pv, *state)
    return pl.pallas_call(
        mix_kernel,
        in_specs=[hbm] * len(operands),
        out_specs=[vmem] * 6,
        out_shape=[
            pltpu.VMEM((half, 2 * RANK), BF16),
            pltpu.VMEM((MESSAGE, W), BF16),
            pltpu.VMEM(pq.shape, BF16),
            pltpu.VMEM(pv.shape, BF16),
            pltpu.VMEM(cq.shape, BF16),
            pltpu.VMEM(cv.shape, BF16),
        ],
        scratch_shapes=[
            pltpu.VMEM((half, width), BF16),
            pltpu.VMEM((ROWS, WQ), F32),
            pltpu.VMEM((ROWS, WV), F32),
            pltpu.VMEM((16, W), F32),
            pltpu.VMEM((16, W), F32),
            pltpu.SemaphoreType.DMA((6,)),
            pltpu.SemaphoreType.DMA((DEPTHS, 3)),
            pltpu.SemaphoreType.DMA((X_BLOCKS - 1,)),
            pltpu.SemaphoreType.DMA((2, 2)),
        ],
        cost_estimate=pl.CostEstimate(
            flops=4 * half * RANK * width, bytes_accessed=14_000_000, transcendentals=0
        ),
        compiler_params=pltpu.CompilerParams(vmem_limit_bytes=24 * 2**20),
        name="mix",
    )(*(in_hbm(a) for a in operands))


def lead_kernel(mixed, swapped, cq, cv, own, to_1, to_2, to_3, total):
    lead = (((0,), (0,)), ((), ()))
    half = mixed.shape[0]
    for n, held in enumerate((mixed, swapped)):
        at = slice(n * half, (n + 1) * half)
        part_q = lax.dot_general(held[:, :RANK], cq[at, :], lead, preferred_element_type=F32)
        part_v = lax.dot_general(held[:, RANK:], cv[at, :], lead, preferred_element_type=F32)
        if n == 0:
            total[:, :WQ] = part_q
            total[:, WQ:] = part_v
        else:
            total[:, :WQ] += part_q
            total[:, WQ:] += part_v
    major, _, per_major, per_minor = own_place()
    for offset, out in enumerate((own, to_1, to_2, to_3)):
        there = lax.rem(major + offset, 4)
        for minor in range(4):
            start = pl.multiple_of((there * per_major + minor * per_minor) * 16, 16)
            out[minor * 16 : (minor + 1) * 16, :] = total[pl.ds(start, 16), :].astype(out.dtype)


def whole_call(body, out, operands, scratch=(), flops=1_000_000):
    vmem = pl.BlockSpec(memory_space=pltpu.VMEM)
    return pl.pallas_call(
        body,
        in_specs=[vmem] * len(operands),
        out_specs=[vmem] * len(out),
        out_shape=[pltpu.VMEM(o.shape, o.dtype) for o in out],
        scratch_shapes=list(scratch),
        cost_estimate=pl.CostEstimate(flops=flops, bytes_accessed=1_000_000, transcendentals=0),
        compiler_params=pltpu.CompilerParams(vmem_limit_bytes=12 * 2**20),
    )(*(in_vmem(a) for a in operands))


def group_kernel(w0, w1, w2, w3, after, out):
    for n, held in enumerate((w0, w1, w2, w3)):
        out[n * ROWS : (n + 1) * ROWS, :] = held[:ROWS, :]


def partial_kernel(own, r1, r2, r3, out):
    out[...] = (own[...] + r1[...].astype(F32) + (r2[...].astype(F32) + r3[...].astype(F32))).astype(BF16)


def moments(low, first, second):
    first_new = beta_first * first + (1.0 - beta_first) * low
    second_new = beta_second * second + (1.0 - beta_second) * low * low
    return first_new, second_new


def update_kernel(own, r1, r2, r3, k0, k1, k2, k3, mq, mv, vq, vv, u, fq, fv, sq, sv, low):
    low[...] = (own[...].astype(F32) + r2[...].astype(F32)) + (r1[...].astype(F32) + r3[...].astype(F32))
    _, minor, _, _ = own_place()
    for offset, held in enumerate((k0, k1, k2, k3)):
        there = lax.rem(minor + 4 - offset, 4)
        at = pl.ds(pl.multiple_of(there * 16, 16), 16)
        first = held[ROWS : ROWS + 16, :].astype(F32)
        second = held[ROWS + 16 :, :].astype(F32)
        first, second = moments(low[at, :], first, second)
        u[at, :] = (first / (jnp.sqrt(second) + adam_eps)).astype(BF16)
    mine = low[pl.ds(pl.multiple_of(minor * 16, 16), 16), :]
    fq[...], sq[...] = moments(mine[:, :WQ], mq[...], vq[...])
    fv[...], sv[...] = moments(mine[:, WQ:], mv[...], vv[...])


def assemble_kernel(own, r1, r2, r3, u, squares):
    major, _, per_major, per_minor = own_place()
    for offset, held in enumerate((own, r1, r2, r3)):
        there = lax.rem(major + 4 - offset, 4)
        for minor in range(4):
            start = pl.multiple_of((there * per_major + minor * per_minor) * 16, 16)
            u[pl.ds(start, 16), :] = held[minor * 16 : (minor + 1) * 16, :]
    total = jnp.zeros((16, W), F32)
    for group in range(16):
        part = u[group * 16 : (group + 1) * 16, :].astype(F32)
        total += part * part
    total = total[:8, :] + total[8:, :]
    folded = total[:, :128]
    for lane in range(1, W // 128):
        folded += total[:, lane * 128 : (lane + 1) * 128]
    squares[...] = folded


def weight_kernel(
    s_own, s_other, u, pq, pv, g0, g1, g2, g3, wq, wv, fq, fv, sq, sv,
    nq, nv, tq, tv, cq, cv, fq_out, fv_out, sq_out, sv_out,
    nq_s, nv_s, tq_s, tv_s, cq_s, cv_s, c_sem, m_sem,
):
    stores = []

    def store(source, target, sem):
        copy = pltpu.make_async_copy(source, target, sem)
        copy.start()
        stores.append(copy)

    for n, (a, b) in enumerate(((fq, fq_out), (fv, fv_out), (sq, sq_out), (sv, sv_out))):
        store(a, b, m_sem.at[n])
    major, minor, per_major, per_minor = own_place()
    squares = jnp.sum(s_own[...] + s_other[...], axis=(0, 1), keepdims=True)
    scale = lax.rsqrt(squares / (RANK * (QK_W + V_W)) + norm_eps)
    uq, uv = u[:, :WQ], u[:, WQ:]
    keep = 1.0 - step_rate * decay_rate
    for i, piece in ((0, g0), (1, g1), (3, g3), (2, g2)):
        a_there = lax.rem(major + 4 - i, 4)
        for j in range(4):
            b_there = lax.rem(minor + 4 - j, 4)
            block = a_there * per_major + b_there * per_minor
            at = pl.ds(pl.multiple_of(block * ROWS, ROWS), ROWS)
            back_q = scale * jnp.dot(pq[at, :], uq, preferred_element_type=F32)
            back_v = scale * jnp.dot(pv[at, :], uv, preferred_element_type=F32)
            held = piece[j * ROWS : (j + 1) * ROWS, :].astype(F32)
            n = i * 4 + j
            cq_s[n] = (keep * held[:, :WQ] - step_rate * back_q).astype(BF16)
            cv_s[n] = (keep * held[:, WQ:] - step_rate * back_v).astype(BF16)
            for part, (source, target) in enumerate(((cq_s, cq), (cv_s, cv))):
                store(source.at[n], target.at[at, :], c_sem.at[n, part])
            if n == 0:
                for back, w, t, new in ((back_q, wq, tq_s, nq_s), (back_v, wv, tv_s, nv_s)):
                    weight = w[...]
                    step = back + decay_rate * weight
                    t[...] = step
                    new[...] = weight - step_rate * step
                for k, (a, b) in enumerate(((nq_s, nq), (nv_s, nv), (tq_s, tq), (tv_s, tv))):
                    store(a, b, m_sem.at[4 + k])
    for copy in stores:
        copy.wait()


def new_weights(s_own, s_other, u, pq, pv, groups, wq, wv, kept):
    vmem = pl.BlockSpec(memory_space=pltpu.VMEM)
    hbm = pl.BlockSpec(memory_space=pl.ANY)
    out = [
        jax.ShapeDtypeStruct((ROWS, WQ), F32),
        jax.ShapeDtypeStruct((ROWS, WV), F32),
        jax.ShapeDtypeStruct((ROWS, WQ), F32),
        jax.ShapeDtypeStruct((ROWS, WV), F32),
        jax.ShapeDtypeStruct((16 * ROWS, WQ), BF16),
        jax.ShapeDtypeStruct((16 * ROWS, WV), BF16),
    ] + [jax.ShapeDtypeStruct(a.shape, F32) for a in kept]
    operands = (s_own, s_other, u, pq, pv, *groups, wq, wv, *kept)
    return pl.pallas_call(
        weight_kernel,
        in_specs=[vmem] * len(operands),
        out_specs=[hbm] * len(out),
        out_shape=out,
        scratch_shapes=[
            pltpu.VMEM((ROWS, WQ), F32),
            pltpu.VMEM((ROWS, WV), F32),
            pltpu.VMEM((ROWS, WQ), F32),
            pltpu.VMEM((ROWS, WV), F32),
            pltpu.VMEM((16, ROWS, WQ), BF16),
            pltpu.VMEM((16, ROWS, WV), BF16),
            pltpu.SemaphoreType.DMA((16, 2)),
            pltpu.SemaphoreType.DMA((8,)),
        ],
        cost_estimate=pl.CostEstimate(
            flops=2 * 16 * ROWS * RANK * W, bytes_accessed=12_000_000, transcendentals=0
        ),
        compiler_params=pltpu.CompilerParams(vmem_limit_bytes=20 * 2**20),
        name="weights",
    )(*(in_vmem(a) for a in operands))


def on_device(inputs, cq, cv, pq, pv, wq, wv, mq, mv, vq, vv):
    mixed, w16, pq, pv, cq, cv = mix(inputs, cq, cv, pq, pv, wq, wv, mq, mv, vq, vv)
    swapped = shifted(mixed, "core", 1)
    w_1, w_2, w_3 = to_all("minor", (w16,) * 3)
    chunk = lambda t: jax.ShapeDtypeStruct((64, W), t)
    own, *parts = whole_call(
        lead_kernel,
        [chunk(F32), chunk(BF16), chunk(BF16), chunk(BF16)],
        (mixed, swapped, cq, cv),
        [pltpu.VMEM((RANK, W), F32)],
        flops=2 * inputs.shape[0] * RANK * W,
    )
    r_1, r_2, r_3 = to_all("major", parts)
    message, = whole_call(
        partial_kernel, [jax.ShapeDtypeStruct((64, W), BF16)], (own, r_1, r_2, r_3)
    )
    m_1, m_2, m_3 = to_all("minor", (message,) * 3)
    group, = whole_call(
        group_kernel, [jax.ShapeDtypeStruct((4 * ROWS, W), BF16)], (w16, w_1, w_2, w_3, message)
    )
    g_3 = shifted(group, "major", 3)
    small = lambda n: jax.ShapeDtypeStruct((16, n), F32)
    u_own, first_q, first_v, second_q, second_v = whole_call(
        update_kernel,
        [jax.ShapeDtypeStruct((64, W), BF16), small(WQ), small(WV), small(WQ), small(WV)],
        (message, m_1, m_2, m_3, w16, w_1, w_2, w_3, mq, mv, vq, vv),
        [pltpu.VMEM((64, W), F32)],
    )
    u_1, u_2, u_3 = to_all("major", (u_own,) * 3)
    g_2 = shifted(g_3, "major", 3)
    g_1 = shifted(group, "major", 1)
    u, squares = whole_call(
        assemble_kernel,
        [jax.ShapeDtypeStruct((RANK, W), BF16), jax.ShapeDtypeStruct((8, 128), F32)],
        (u_own, u_1, u_2, u_3),
    )
    s_1, s_2, s_3 = to_all("x", (squares,) * 3)
    chips = (squares + s_2) + (s_1 + s_3)
    other = shifted(chips, "core", 1)
    kept = (first_q, first_v, second_q, second_v)
    new_q, new_v, step_q, step_v, copy_q, copy_v, *kept = new_weights(
        chips, other, u, pq, pv, (group, g_1, g_2, g_3), wq, wv, kept
    )
    return (new_q, new_v, copy_q, copy_v, *kept, step_q, step_v)


def solution(mesh):
    finer = Mesh(mesh.devices.reshape(SIZES), AXES)
    both, tokens, columns = P(FS, TP), P(FS, None), P(None, TP)
    return jax.shard_map(
        on_device,
        mesh=finer,
        in_specs=(tokens, both, both, P(), P()) + (both,) * 6,
        out_specs=(both, both, columns, columns) + (both,) * 6,
        check_vma=False,
    )
```

```python
import jax
import jax.numpy as jnp
from jax import lax
from jax.experimental import pallas as pl
from jax.experimental.pallas import tpu as pltpu
from jax.sharding import Mesh
from jax.sharding import PartitionSpec as P

RANK = 256
QK_W = 2048
V_W = 4096
AXES = ("z", "y", "x", "c")
SIZES = (4, 4, 4, 2)
FS = ("z", "y")
TP = ("x", "c")

beta_first = 0.9
beta_second = 0.95
adam_eps = 1e-08
norm_eps = 1e-06
step_rate = 0.05
decay_rate = 0.2

WQ = 256
WV = 512
W = WQ + WV
ROWS = 128
MESSAGE = ROWS + 32
X_BLOCKS = 3
DEPTHS = 4

F32 = jnp.float32
BF16 = jnp.bfloat16


def shift_pairs(kind, offset):
    pairs = []
    for z in range(4):
        for y in range(4):
            for x in range(4):
                for c in range(2):
                    to = [z, y, x, c]
                    if kind == "major":
                        axis = 0 if c == 0 else 1
                    elif kind == "minor":
                        axis = 1 if c == 0 else 0
                    elif kind == "x":
                        axis = 2
                    else:
                        axis = 3
                    to[axis] = (to[axis] + offset) % SIZES[axis]
                    source = ((z * 4 + y) * 4 + x) * 2 + c
                    target = ((to[0] * 4 + to[1]) * 4 + to[2]) * 2 + to[3]
                    pairs.append((source, target))
    return pairs


def shifted(array, kind, offset):
    return lax.ppermute(array, AXES, shift_pairs(kind, offset))


def to_all(kind, arrays):
    two = shifted(arrays[1], kind, 2)
    return shifted(arrays[0], kind, 1), two, shifted(arrays[2], kind, 3)


def own_place():
    z, y, c = lax.axis_index("z"), lax.axis_index("y"), lax.axis_index("c")
    first = c == 0
    major = jnp.where(first, z, y)
    minor = jnp.where(first, y, z)
    per_major = jnp.where(first, 4, 1)
    per_minor = jnp.where(first, 1, 4)
    return major, minor, per_major, per_minor


def in_vmem(array):
    return pltpu.with_memory_space_constraint(array, pltpu.VMEM)


def in_hbm(array):
    return pltpu.with_memory_space_constraint(array, pltpu.HBM)


def mix_kernel(
    x, cq, cv, pq, pv, wq, wv, mq, mv, vq, vv,
    mixed, w16, pq_out, pv_out, cq_out, cv_out,
    xs, wq_s, wv_s, m_s, v_s, sem, p_sem, x_sem, c_sem,
):
    half, block = mixed.shape[0], xs.shape[0] // X_BLOCKS
    core = lax.axis_index("c")
    mine = pl.multiple_of(core * half, half)
    other = pl.multiple_of((1 - core) * half, half)
    depth = pq.shape[0] // DEPTHS
    parts = [pl.ds(k * depth, depth) for k in range(DEPTHS)]
    first = [
        [
            pltpu.make_async_copy(pq.at[k, :], pq_out.at[k, :], p_sem.at[n, 0]),
            pltpu.make_async_copy(pv.at[k, :], pv_out.at[k, :], p_sem.at[n, 1]),
            pltpu.make_async_copy(x.at[pl.ds(mine, block), k], xs.at[pl.ds(0, block), k], p_sem.at[n, 2]),
        ]
        for n, k in enumerate(parts)
    ]
    blocks = [
        pltpu.make_async_copy(
            x.at[pl.ds(mine + n * block, block), :], xs.at[pl.ds(n * block, block), :], x_sem.at[n - 1]
        )
        for n in range(1, X_BLOCKS)
    ]
    pairs = (
        (wq, wq_s),
        (wv, wv_s),
        (mq, m_s.at[:, pl.ds(0, WQ)]),
        (mv, m_s.at[:, pl.ds(WQ, WV)]),
        (vq, v_s.at[:, pl.ds(0, WQ)]),
        (vv, v_s.at[:, pl.ds(WQ, WV)]),
    )
    small = [pltpu.make_async_copy(a, b, sem.at[n]) for n, (a, b) in enumerate(pairs)]
    cotangents = [
        pltpu.make_async_copy(
            a.at[pl.ds(start, half), :], b.at[pl.ds(at * half, half), :], c_sem.at[n, at]
        )
        for n, (a, b) in enumerate(((cq, cq_out), (cv, cv_out)))
        for at, start in enumerate((mine, other))
    ]
    for copy in (*(c for piece in first for c in piece), *blocks):
        copy.start()
    part_q = part_v = None
    for piece, k in zip(first, parts):
        for copy in piece:
            copy.wait()
        rows = xs[:block, k]
        piece_q = jnp.dot(rows, pq_out[k, :], preferred_element_type=F32)
        piece_v = jnp.dot(rows, pv_out[k, :], preferred_element_type=F32)
        part_q = piece_q if part_q is None else part_q + piece_q
        part_v = piece_v if part_v is None else part_v + piece_v
    for copy in (*small, *cotangents):
        copy.start()
    mixed[:block, :RANK] = part_q.astype(BF16)
    mixed[:block, RANK:] = part_v.astype(BF16)
    for n in range(1, X_BLOCKS):
        blocks[n - 1].wait()
        at = slice(n * block, (n + 1) * block)
        rows = xs[at, :]
        mixed[at, :RANK] = jnp.dot(rows, pq_out[...], preferred_element_type=F32).astype(BF16)
        mixed[at, RANK:] = jnp.dot(rows, pv_out[...], preferred_element_type=F32).astype(BF16)
    for copy in small:
        copy.wait()
    w16[:ROWS, :WQ] = wq_s[...].astype(BF16)
    w16[:ROWS, WQ:] = wv_s[...].astype(BF16)
    w16[ROWS : ROWS + 16, :] = m_s[...].astype(BF16)
    w16[ROWS + 16 :, :] = v_s[...].astype(BF16)
    for copy in cotangents:
        copy.wait()


def mix(inputs, cq, cv, pq, pv, *state):
    vmem, hbm = pl.BlockSpec(memory_space=pltpu.VMEM), pl.BlockSpec(memory_space=pl.ANY)
    tokens, width = inputs.shape
    half = tokens // 2
    operands = (inputs, cq, cv, pq, pv, *state)
    return pl.pallas_call(
        mix_kernel,
        in_specs=[hbm] * len(operands),
        out_specs=[vmem] * 6,
        out_shape=[
            pltpu.VMEM((half, 2 * RANK), BF16),
            pltpu.VMEM((MESSAGE, W), BF16),
            pltpu.VMEM(pq.shape, BF16),
            pltpu.VMEM(pv.shape, BF16),
            pltpu.VMEM(cq.shape, BF16),
            pltpu.VMEM(cv.shape, BF16),
        ],
        scratch_shapes=[
            pltpu.VMEM((half, width), BF16),
            pltpu.VMEM((ROWS, WQ), F32),
            pltpu.VMEM((ROWS, WV), F32),
            pltpu.VMEM((16, W), F32),
            pltpu.VMEM((16, W), F32),
            pltpu.SemaphoreType.DMA((6,)),
            pltpu.SemaphoreType.DMA((DEPTHS, 3)),
            pltpu.SemaphoreType.DMA((X_BLOCKS - 1,)),
            pltpu.SemaphoreType.DMA((2, 2)),
        ],
        cost_estimate=pl.CostEstimate(
            flops=4 * half * RANK * width, bytes_accessed=14_000_000, transcendentals=0
        ),
        compiler_params=pltpu.CompilerParams(vmem_limit_bytes=24 * 2**20),
        name="mix",
    )(*(in_hbm(a) for a in operands))


def lead_kernel(mixed, swapped, cq, cv, own, to_1, to_2, to_3, total):
    lead = (((0,), (0,)), ((), ()))
    half = mixed.shape[0]
    for n, held in enumerate((mixed, swapped)):
        at = slice(n * half, (n + 1) * half)
        part_q = lax.dot_general(held[:, :RANK], cq[at, :], lead, preferred_element_type=F32)
        part_v = lax.dot_general(held[:, RANK:], cv[at, :], lead, preferred_element_type=F32)
        if n == 0:
            total[:, :WQ] = part_q
            total[:, WQ:] = part_v
        else:
            total[:, :WQ] += part_q
            total[:, WQ:] += part_v
    major, _, per_major, per_minor = own_place()
    for offset, out in enumerate((own, to_1, to_2, to_3)):
        there = lax.rem(major + offset, 4)
        for minor in range(4):
            start = pl.multiple_of((there * per_major + minor * per_minor) * 16, 16)
            out[minor * 16 : (minor + 1) * 16, :] = total[pl.ds(start, 16), :].astype(out.dtype)


def whole_call(body, out, operands, scratch=(), flops=1_000_000):
    vmem = pl.BlockSpec(memory_space=pltpu.VMEM)
    return pl.pallas_call(
        body,
        in_specs=[vmem] * len(operands),
        out_specs=[vmem] * len(out),
        out_shape=[pltpu.VMEM(o.shape, o.dtype) for o in out],
        scratch_shapes=list(scratch),
        cost_estimate=pl.CostEstimate(flops=flops, bytes_accessed=1_000_000, transcendentals=0),
        compiler_params=pltpu.CompilerParams(vmem_limit_bytes=12 * 2**20),
    )(*(in_vmem(a) for a in operands))


def group_kernel(w0, w1, w2, w3, after, out):
    for n, held in enumerate((w0, w1, w2, w3)):
        out[n * ROWS : (n + 1) * ROWS, :] = held[:ROWS, :]


def partial_kernel(own, r1, r2, r3, out):
    out[...] = (own[...] + r1[...].astype(F32) + (r2[...].astype(F32) + r3[...].astype(F32))).astype(BF16)


def moments(low, first, second):
    first_new = beta_first * first + (1.0 - beta_first) * low
    second_new = beta_second * second + (1.0 - beta_second) * low * low
    return first_new, second_new


def update_kernel(own, r1, r2, r3, k0, k1, k2, k3, mq, mv, vq, vv, u, fq, fv, sq, sv, low):
    low[...] = (own[...].astype(F32) + r2[...].astype(F32)) + (r1[...].astype(F32) + r3[...].astype(F32))
    _, minor, _, _ = own_place()
    for offset, held in enumerate((k0, k1, k2, k3)):
        there = lax.rem(minor + 4 - offset, 4)
        at = pl.ds(pl.multiple_of(there * 16, 16), 16)
        first = held[ROWS : ROWS + 16, :].astype(F32)
        second = held[ROWS + 16 :, :].astype(F32)
        first, second = moments(low[at, :], first, second)
        u[at, :] = (first / (jnp.sqrt(second) + adam_eps)).astype(BF16)
    mine = low[pl.ds(pl.multiple_of(minor * 16, 16), 16), :]
    fq[...], sq[...] = moments(mine[:, :WQ], mq[...], vq[...])
    fv[...], sv[...] = moments(mine[:, WQ:], mv[...], vv[...])


def assemble_kernel(own, r1, r2, r3, u, squares):
    major, _, per_major, per_minor = own_place()
    for offset, held in enumerate((own, r1, r2, r3)):
        there = lax.rem(major + 4 - offset, 4)
        for minor in range(4):
            start = pl.multiple_of((there * per_major + minor * per_minor) * 16, 16)
            u[pl.ds(start, 16), :] = held[minor * 16 : (minor + 1) * 16, :]
    total = jnp.zeros((16, W), F32)
    for group in range(16):
        part = u[group * 16 : (group + 1) * 16, :].astype(F32)
        total += part * part
    total = total[:8, :] + total[8:, :]
    folded = total[:, :128]
    for lane in range(1, W // 128):
        folded += total[:, lane * 128 : (lane + 1) * 128]
    squares[...] = folded


def back_kernel(u, pq, pv, back):
    for n in range(4):
        at = slice(n * 4 * ROWS, (n + 1) * 4 * ROWS)
        back[at, :WQ] = jnp.dot(pq[at, :], u[:, :WQ], preferred_element_type=F32)
        back[at, WQ:] = jnp.dot(pv[at, :], u[:, WQ:], preferred_element_type=F32)


def weight_kernel(
    s_own, s_other, back, g0, g1, g2, g3, wq, wv, fq, fv, sq, sv,
    nq, nv, tq, tv, cq, cv, fq_out, fv_out, sq_out, sv_out,
    nq_s, nv_s, tq_s, tv_s, cq_s, cv_s, c_sem, m_sem,
):
    stores = []

    def store(source, target, sem):
        copy = pltpu.make_async_copy(source, target, sem)
        copy.start()
        stores.append(copy)

    for n, (a, b) in enumerate(((fq, fq_out), (fv, fv_out), (sq, sq_out), (sv, sv_out))):
        store(a, b, m_sem.at[n])
    major, minor, per_major, per_minor = own_place()
    squares = jnp.sum(s_own[...] + s_other[...], axis=(0, 1), keepdims=True)
    scale = lax.rsqrt(squares / (RANK * (QK_W + V_W)) + norm_eps)
    keep = 1.0 - step_rate * decay_rate
    for i, piece in ((0, g0), (1, g1), (3, g3), (2, g2)):
        a_there = lax.rem(major + 4 - i, 4)
        for j in range(4):
            b_there = lax.rem(minor + 4 - j, 4)
            block = a_there * per_major + b_there * per_minor
            at = pl.ds(pl.multiple_of(block * ROWS, ROWS), ROWS)
            back_q = scale * back[at, :WQ]
            back_v = scale * back[at, WQ:]
            held = piece[j * ROWS : (j + 1) * ROWS, :].astype(F32)
            n = i * 4 + j
            cq_s[n] = (keep * held[:, :WQ] - step_rate * back_q).astype(BF16)
            cv_s[n] = (keep * held[:, WQ:] - step_rate * back_v).astype(BF16)
            for part, (source, target) in enumerate(((cq_s, cq), (cv_s, cv))):
                store(source.at[n], target.at[at, :], c_sem.at[n, part])
            if n == 0:
                for scaled, w, t, new in ((back_q, wq, tq_s, nq_s), (back_v, wv, tv_s, nv_s)):
                    weight = w[...]
                    step = scaled + decay_rate * weight
                    t[...] = step
                    new[...] = weight - step_rate * step
                for k, (a, b) in enumerate(((nq_s, nq), (nv_s, nv), (tq_s, tq), (tv_s, tv))):
                    store(a, b, m_sem.at[4 + k])
    for copy in stores:
        copy.wait()


def new_weights(s_own, s_other, back, groups, wq, wv, kept):
    vmem = pl.BlockSpec(memory_space=pltpu.VMEM)
    hbm = pl.BlockSpec(memory_space=pl.ANY)
    out = [
        jax.ShapeDtypeStruct((ROWS, WQ), F32),
        jax.ShapeDtypeStruct((ROWS, WV), F32),
        jax.ShapeDtypeStruct((ROWS, WQ), F32),
        jax.ShapeDtypeStruct((ROWS, WV), F32),
        jax.ShapeDtypeStruct((16 * ROWS, WQ), BF16),
        jax.ShapeDtypeStruct((16 * ROWS, WV), BF16),
    ] + [jax.ShapeDtypeStruct(a.shape, F32) for a in kept]
    operands = (s_own, s_other, back, *groups, wq, wv, *kept)
    return pl.pallas_call(
        weight_kernel,
        in_specs=[vmem] * len(operands),
        out_specs=[hbm] * len(out),
        out_shape=out,
        scratch_shapes=[
            pltpu.VMEM((ROWS, WQ), F32),
            pltpu.VMEM((ROWS, WV), F32),
            pltpu.VMEM((ROWS, WQ), F32),
            pltpu.VMEM((ROWS, WV), F32),
            pltpu.VMEM((16, ROWS, WQ), BF16),
            pltpu.VMEM((16, ROWS, WV), BF16),
            pltpu.SemaphoreType.DMA((16, 2)),
            pltpu.SemaphoreType.DMA((8,)),
        ],
        cost_estimate=pl.CostEstimate(
            flops=16 * ROWS * W * 4, bytes_accessed=12_000_000, transcendentals=0
        ),
        compiler_params=pltpu.CompilerParams(vmem_limit_bytes=20 * 2**20),
        name="weights",
    )(*(in_vmem(a) for a in operands))


def on_device(inputs, cq, cv, pq, pv, wq, wv, mq, mv, vq, vv):
    mixed, w16, pq, pv, cq, cv = mix(inputs, cq, cv, pq, pv, wq, wv, mq, mv, vq, vv)
    swapped = shifted(mixed, "core", 1)
    w_1, w_2, w_3 = to_all("minor", (w16,) * 3)
    chunk = lambda t: jax.ShapeDtypeStruct((64, W), t)
    own, *parts = whole_call(
        lead_kernel,
        [chunk(F32), chunk(BF16), chunk(BF16), chunk(BF16)],
        (mixed, swapped, cq, cv),
        [pltpu.VMEM((RANK, W), F32)],
        flops=2 * inputs.shape[0] * RANK * W,
    )
    r_1, r_2, r_3 = to_all("major", parts)
    group, = whole_call(
        group_kernel, [jax.ShapeDtypeStruct((4 * ROWS, W), BF16)], (w16, w_1, w_2, w_3, own)
    )
    g_3 = shifted(group, "major", 3)
    message, = whole_call(
        partial_kernel, [jax.ShapeDtypeStruct((64, W), BF16)], (own, r_1, r_2, r_3)
    )
    m_1, m_2, m_3 = to_all("minor", (message,) * 3)
    small = lambda n: jax.ShapeDtypeStruct((16, n), F32)
    u_own, first_q, first_v, second_q, second_v = whole_call(
        update_kernel,
        [jax.ShapeDtypeStruct((64, W), BF16), small(WQ), small(WV), small(WQ), small(WV)],
        (message, m_1, m_2, m_3, w16, w_1, w_2, w_3, mq, mv, vq, vv),
        [pltpu.VMEM((64, W), F32)],
    )
    u_1, u_2, u_3 = to_all("major", (u_own,) * 3)
    g_2 = shifted(g_3, "major", 3)
    g_1 = shifted(group, "major", 1)
    u, squares = whole_call(
        assemble_kernel,
        [jax.ShapeDtypeStruct((RANK, W), BF16), jax.ShapeDtypeStruct((8, 128), F32)],
        (u_own, u_1, u_2, u_3),
    )
    s_1, s_2, s_3 = to_all("x", (squares,) * 3)
    back, = whole_call(
        back_kernel,
        [jax.ShapeDtypeStruct((16 * ROWS, W), F32)],
        (u, pq, pv),
        flops=2 * 16 * ROWS * RANK * W,
    )
    chips = (squares + s_2) + (s_1 + s_3)
    other = shifted(chips, "core", 1)
    kept = (first_q, first_v, second_q, second_v)
    new_q, new_v, step_q, step_v, copy_q, copy_v, *kept = new_weights(
        chips, other, back, (group, g_1, g_2, g_3), wq, wv, kept
    )
    return (new_q, new_v, copy_q, copy_v, *kept, step_q, step_v)


def solution(mesh):
    finer = Mesh(mesh.devices.reshape(SIZES), AXES)
    both, tokens, columns = P(FS, TP), P(FS, None), P(None, TP)
    return jax.shard_map(
        on_device,
        mesh=finer,
        in_specs=(tokens, both, both, P(), P()) + (both,) * 6,
        out_specs=(both, both, columns, columns) + (both,) * 6,
        check_vma=False,
    )
```

```python
import jax
import jax.numpy as jnp
from jax import lax
from jax.experimental import pallas as pl
from jax.experimental.pallas import tpu as pltpu
from jax.sharding import Mesh
from jax.sharding import PartitionSpec as P

RANK = 256
QK_W = 2048
V_W = 4096
AXES = ("z", "y", "x", "c")
SIZES = (4, 4, 4, 2)
FS = ("z", "y")
TP = ("x", "c")

beta_first = 0.9
beta_second = 0.95
adam_eps = 1e-08
norm_eps = 1e-06
step_rate = 0.05
decay_rate = 0.2

WQ = 256
WV = 512
W = WQ + WV
ROWS = 128
MESSAGE = ROWS + 32
X_BLOCKS = 3
DEPTHS = 4

F32 = jnp.float32
BF16 = jnp.bfloat16


def shift_pairs(kind, offset):
    pairs = []
    for z in range(4):
        for y in range(4):
            for x in range(4):
                for c in range(2):
                    to = [z, y, x, c]
                    if kind == "major":
                        axis = 0 if c == 0 else 1
                    elif kind == "minor":
                        axis = 1 if c == 0 else 0
                    elif kind == "x":
                        axis = 2
                    else:
                        axis = 3
                    to[axis] = (to[axis] + offset) % SIZES[axis]
                    source = ((z * 4 + y) * 4 + x) * 2 + c
                    target = ((to[0] * 4 + to[1]) * 4 + to[2]) * 2 + to[3]
                    pairs.append((source, target))
    return pairs


def shifted(array, kind, offset):
    return lax.ppermute(array, AXES, shift_pairs(kind, offset))


def to_all(kind, arrays):
    two = shifted(arrays[1], kind, 2)
    return shifted(arrays[0], kind, 1), two, shifted(arrays[2], kind, 3)


def own_place():
    z, y, c = lax.axis_index("z"), lax.axis_index("y"), lax.axis_index("c")
    first = c == 0
    major = jnp.where(first, z, y)
    minor = jnp.where(first, y, z)
    per_major = jnp.where(first, 4, 1)
    per_minor = jnp.where(first, 1, 4)
    return major, minor, per_major, per_minor


def in_vmem(array):
    return pltpu.with_memory_space_constraint(array, pltpu.VMEM)


def in_hbm(array):
    return pltpu.with_memory_space_constraint(array, pltpu.HBM)


def mix_kernel(
    x, cq, cv, pq, pv, wq, wv, mq, mv, vq, vv,
    mixed, w16, pq_out, pv_out, cq_out, cv_out,
    xs, wq_s, wv_s, m_s, v_s, sem, p_sem, x_sem, c_sem,
):
    half, block = mixed.shape[0], xs.shape[0] // X_BLOCKS
    core = lax.axis_index("c")
    mine = pl.multiple_of(core * half, half)
    other = pl.multiple_of((1 - core) * half, half)
    depth = pq.shape[0] // DEPTHS
    parts = [pl.ds(k * depth, depth) for k in range(DEPTHS)]
    first = [
        [
            pltpu.make_async_copy(pq.at[k, :], pq_out.at[k, :], p_sem.at[n, 0]),
            pltpu.make_async_copy(pv.at[k, :], pv_out.at[k, :], p_sem.at[n, 1]),
            pltpu.make_async_copy(x.at[pl.ds(mine, block), k], xs.at[pl.ds(0, block), k], p_sem.at[n, 2]),
        ]
        for n, k in enumerate(parts)
    ]
    blocks = [
        pltpu.make_async_copy(
            x.at[pl.ds(mine + n * block, block), :], xs.at[pl.ds(n * block, block), :], x_sem.at[n - 1]
        )
        for n in range(1, X_BLOCKS)
    ]
    pairs = (
        (wq, wq_s),
        (wv, wv_s),
        (mq, m_s.at[:, pl.ds(0, WQ)]),
        (mv, m_s.at[:, pl.ds(WQ, WV)]),
        (vq, v_s.at[:, pl.ds(0, WQ)]),
        (vv, v_s.at[:, pl.ds(WQ, WV)]),
    )
    small = [pltpu.make_async_copy(a, b, sem.at[n]) for n, (a, b) in enumerate(pairs)]
    cotangents = [
        pltpu.make_async_copy(
            a.at[pl.ds(start, half), :], b.at[pl.ds(at * half, half), :], c_sem.at[n, at]
        )
        for n, (a, b) in enumerate(((cq, cq_out), (cv, cv_out)))
        for at, start in enumerate((mine, other))
    ]
    for copy in (*(c for piece in first for c in piece), *blocks):
        copy.start()
    part_q = part_v = None
    for piece, k in zip(first, parts):
        for copy in piece:
            copy.wait()
        rows = xs[:block, k]
        piece_q = jnp.dot(rows, pq_out[k, :], preferred_element_type=F32)
        piece_v = jnp.dot(rows, pv_out[k, :], preferred_element_type=F32)
        part_q = piece_q if part_q is None else part_q + piece_q
        part_v = piece_v if part_v is None else part_v + piece_v
    for copy in (*small, *cotangents):
        copy.start()
    mixed[:block, :RANK] = part_q.astype(BF16)
    mixed[:block, RANK:] = part_v.astype(BF16)
    for n in range(1, X_BLOCKS):
        blocks[n - 1].wait()
        at = slice(n * block, (n + 1) * block)
        rows = xs[at, :]
        mixed[at, :RANK] = jnp.dot(rows, pq_out[...], preferred_element_type=F32).astype(BF16)
        mixed[at, RANK:] = jnp.dot(rows, pv_out[...], preferred_element_type=F32).astype(BF16)
    for copy in small:
        copy.wait()
    w16[:ROWS, :WQ] = wq_s[...].astype(BF16)
    w16[:ROWS, WQ:] = wv_s[...].astype(BF16)
    w16[ROWS : ROWS + 16, :] = m_s[...].astype(BF16)
    w16[ROWS + 16 :, :] = v_s[...].astype(BF16)
    for copy in cotangents:
        copy.wait()


def mix(inputs, cq, cv, pq, pv, *state):
    vmem, hbm = pl.BlockSpec(memory_space=pltpu.VMEM), pl.BlockSpec(memory_space=pl.ANY)
    tokens, width = inputs.shape
    half = tokens // 2
    operands = (inputs, cq, cv, pq, pv, *state)
    return pl.pallas_call(
        mix_kernel,
        in_specs=[hbm] * len(operands),
        out_specs=[vmem] * 6,
        out_shape=[
            pltpu.VMEM((half, 2 * RANK), BF16),
            pltpu.VMEM((MESSAGE, W), BF16),
            pltpu.VMEM(pq.shape, BF16),
            pltpu.VMEM(pv.shape, BF16),
            pltpu.VMEM(cq.shape, BF16),
            pltpu.VMEM(cv.shape, BF16),
        ],
        scratch_shapes=[
            pltpu.VMEM((half, width), BF16),
            pltpu.VMEM((ROWS, WQ), F32),
            pltpu.VMEM((ROWS, WV), F32),
            pltpu.VMEM((16, W), F32),
            pltpu.VMEM((16, W), F32),
            pltpu.SemaphoreType.DMA((6,)),
            pltpu.SemaphoreType.DMA((DEPTHS, 3)),
            pltpu.SemaphoreType.DMA((X_BLOCKS - 1,)),
            pltpu.SemaphoreType.DMA((2, 2)),
        ],
        cost_estimate=pl.CostEstimate(
            flops=4 * half * RANK * width, bytes_accessed=14_000_000, transcendentals=0
        ),
        compiler_params=pltpu.CompilerParams(vmem_limit_bytes=24 * 2**20),
        name="mix",
    )(*(in_hbm(a) for a in operands))


def lead_kernel(mixed, swapped, cq, cv, own, to_1, to_2, to_3, total):
    lead = (((0,), (0,)), ((), ()))
    half = mixed.shape[0]
    for n, held in enumerate((mixed, swapped)):
        at = slice(n * half, (n + 1) * half)
        part_q = lax.dot_general(held[:, :RANK], cq[at, :], lead, preferred_element_type=F32)
        part_v = lax.dot_general(held[:, RANK:], cv[at, :], lead, preferred_element_type=F32)
        if n == 0:
            total[:, :WQ] = part_q
            total[:, WQ:] = part_v
        else:
            total[:, :WQ] += part_q
            total[:, WQ:] += part_v
    major, _, per_major, per_minor = own_place()
    for offset, out in enumerate((own, to_1, to_2, to_3)):
        there = lax.rem(major + offset, 4)
        for minor in range(4):
            start = pl.multiple_of((there * per_major + minor * per_minor) * 16, 16)
            out[minor * 16 : (minor + 1) * 16, :] = total[pl.ds(start, 16), :].astype(out.dtype)


def whole_call(body, out, operands, scratch=(), flops=1_000_000):
    vmem = pl.BlockSpec(memory_space=pltpu.VMEM)
    return pl.pallas_call(
        body,
        in_specs=[vmem] * len(operands),
        out_specs=[vmem] * len(out),
        out_shape=[pltpu.VMEM(o.shape, o.dtype) for o in out],
        scratch_shapes=list(scratch),
        cost_estimate=pl.CostEstimate(flops=flops, bytes_accessed=1_000_000, transcendentals=0),
        compiler_params=pltpu.CompilerParams(vmem_limit_bytes=12 * 2**20),
    )(*(in_vmem(a) for a in operands))


def group_kernel(w0, w1, w2, w3, after, out):
    for n, held in enumerate((w0, w1, w2, w3)):
        out[n * ROWS : (n + 1) * ROWS, :] = held[:ROWS, :]


def partial_kernel(own, r1, r2, r3, out):
    out[...] = (own[...] + r1[...].astype(F32) + (r2[...].astype(F32) + r3[...].astype(F32))).astype(BF16)


def moments(low, first, second):
    first_new = beta_first * first + (1.0 - beta_first) * low
    second_new = beta_second * second + (1.0 - beta_second) * low * low
    return first_new, second_new


def update_kernel(own, r1, r2, r3, k0, k1, k2, k3, mq, mv, vq, vv, u, fq, fv, sq, sv, low):
    low[...] = (own[...].astype(F32) + r2[...].astype(F32)) + (r1[...].astype(F32) + r3[...].astype(F32))
    _, minor, _, _ = own_place()
    for offset, held in enumerate((k0, k1, k2, k3)):
        there = lax.rem(minor + 4 - offset, 4)
        at = pl.ds(pl.multiple_of(there * 16, 16), 16)
        first = held[ROWS : ROWS + 16, :].astype(F32)
        second = held[ROWS + 16 :, :].astype(F32)
        first, second = moments(low[at, :], first, second)
        u[at, :] = (first / (jnp.sqrt(second) + adam_eps)).astype(BF16)
    mine = low[pl.ds(pl.multiple_of(minor * 16, 16), 16), :]
    fq[...], sq[...] = moments(mine[:, :WQ], mq[...], vq[...])
    fv[...], sv[...] = moments(mine[:, WQ:], mv[...], vv[...])


def assemble_kernel(own, r1, r2, r3, u, squares):
    major, _, per_major, per_minor = own_place()
    for offset, held in enumerate((own, r1, r2, r3)):
        there = lax.rem(major + 4 - offset, 4)
        for minor in range(4):
            start = pl.multiple_of((there * per_major + minor * per_minor) * 16, 16)
            u[pl.ds(start, 16), :] = held[minor * 16 : (minor + 1) * 16, :]
    total = jnp.zeros((16, W), F32)
    for group in range(16):
        part = u[group * 16 : (group + 1) * 16, :].astype(F32)
        total += part * part
    total = total[:8, :] + total[8:, :]
    folded = total[:, :128]
    for lane in range(1, W // 128):
        folded += total[:, lane * 128 : (lane + 1) * 128]
    squares[...] = folded


def weight_kernel(
    s_own, s_other, u, pq, pv, g0, g1, g2, g3, wq, wv, fq, fv, sq, sv,
    nq, nv, tq, tv, cq, cv, fq_out, fv_out, sq_out, sv_out,
    nq_s, nv_s, tq_s, tv_s, cq_s, cv_s, c_sem, m_sem,
):
    stores = []

    def store(source, target, sem):
        copy = pltpu.make_async_copy(source, target, sem)
        copy.start()
        stores.append(copy)

    for n, (a, b) in enumerate(((fq, fq_out), (fv, fv_out), (sq, sq_out), (sv, sv_out))):
        store(a, b, m_sem.at[n])
    major, minor, per_major, per_minor = own_place()
    squares = jnp.sum(s_own[...] + s_other[...], axis=(0, 1), keepdims=True)
    scale = lax.rsqrt(squares / (RANK * (QK_W + V_W)) + norm_eps)
    uq, uv = u[:, :WQ], u[:, WQ:]
    keep = 1.0 - step_rate * decay_rate
    for i, piece in ((0, g0), (1, g1), (3, g3), (2, g2)):
        a_there = lax.rem(major + 4 - i, 4)
        for j in range(4):
            b_there = lax.rem(minor + 4 - j, 4)
            block = a_there * per_major + b_there * per_minor
            at = pl.ds(pl.multiple_of(block * ROWS, ROWS), ROWS)
            back_q = scale * jnp.dot(pq[at, :], uq, preferred_element_type=F32)
            back_v = scale * jnp.dot(pv[at, :], uv, preferred_element_type=F32)
            held = piece[j * ROWS : (j + 1) * ROWS, :].astype(F32)
            n = i * 4 + j
            cq_s[n] = (keep * held[:, :WQ] - step_rate * back_q).astype(BF16)
            cv_s[n] = (keep * held[:, WQ:] - step_rate * back_v).astype(BF16)
            for part, (source, target) in enumerate(((cq_s, cq), (cv_s, cv))):
                store(source.at[n], target.at[at, :], c_sem.at[n, part])
            if n == 0:
                for back, w, t, new in ((back_q, wq, tq_s, nq_s), (back_v, wv, tv_s, nv_s)):
                    weight = w[...]
                    step = back + decay_rate * weight
                    t[...] = step
                    new[...] = weight - step_rate * step
                for k, (a, b) in enumerate(((nq_s, nq), (nv_s, nv), (tq_s, tq), (tv_s, tv))):
                    store(a, b, m_sem.at[4 + k])
    for copy in stores:
        copy.wait()


def new_weights(s_own, s_other, u, pq, pv, groups, wq, wv, kept):
    vmem = pl.BlockSpec(memory_space=pltpu.VMEM)
    hbm = pl.BlockSpec(memory_space=pl.ANY)
    out = [
        jax.ShapeDtypeStruct((ROWS, WQ), F32),
        jax.ShapeDtypeStruct((ROWS, WV), F32),
        jax.ShapeDtypeStruct((ROWS, WQ), F32),
        jax.ShapeDtypeStruct((ROWS, WV), F32),
        jax.ShapeDtypeStruct((16 * ROWS, WQ), BF16),
        jax.ShapeDtypeStruct((16 * ROWS, WV), BF16),
    ] + [jax.ShapeDtypeStruct(a.shape, F32) for a in kept]
    operands = (s_own, s_other, u, pq, pv, *groups, wq, wv, *kept)
    return pl.pallas_call(
        weight_kernel,
        in_specs=[vmem] * len(operands),
        out_specs=[hbm] * len(out),
        out_shape=out,
        scratch_shapes=[
            pltpu.VMEM((ROWS, WQ), F32),
            pltpu.VMEM((ROWS, WV), F32),
            pltpu.VMEM((ROWS, WQ), F32),
            pltpu.VMEM((ROWS, WV), F32),
            pltpu.VMEM((16, ROWS, WQ), BF16),
            pltpu.VMEM((16, ROWS, WV), BF16),
            pltpu.SemaphoreType.DMA((16, 2)),
            pltpu.SemaphoreType.DMA((8,)),
        ],
        cost_estimate=pl.CostEstimate(
            flops=2 * 16 * ROWS * RANK * W, bytes_accessed=12_000_000, transcendentals=0
        ),
        compiler_params=pltpu.CompilerParams(vmem_limit_bytes=20 * 2**20),
        name="weights",
    )(*(in_vmem(a) for a in operands))


def on_device(inputs, cq, cv, pq, pv, wq, wv, mq, mv, vq, vv):
    mixed, w16, pq, pv, cq, cv = mix(inputs, cq, cv, pq, pv, wq, wv, mq, mv, vq, vv)
    swapped = shifted(mixed, "core", 1)
    w_1, w_3 = shifted(w16, "minor", 1), shifted(w16, "minor", 3)
    w_2 = shifted(w_3, "minor", 3)
    chunk = lambda t: jax.ShapeDtypeStruct((64, W), t)
    own, *parts = whole_call(
        lead_kernel,
        [chunk(F32), chunk(BF16), chunk(BF16), chunk(BF16)],
        (mixed, swapped, cq, cv),
        [pltpu.VMEM((RANK, W), F32)],
        flops=2 * inputs.shape[0] * RANK * W,
    )
    r_1, r_2, r_3 = to_all("major", parts)
    group, = whole_call(
        group_kernel, [jax.ShapeDtypeStruct((4 * ROWS, W), BF16)], (w16, w_1, w_2, w_3, own)
    )
    g_3 = shifted(group, "major", 3)
    message, = whole_call(
        partial_kernel, [jax.ShapeDtypeStruct((64, W), BF16)], (own, r_1, r_2, r_3)
    )
    m_1, m_2, m_3 = to_all("minor", (message,) * 3)
    small = lambda n: jax.ShapeDtypeStruct((16, n), F32)
    u_own, first_q, first_v, second_q, second_v = whole_call(
        update_kernel,
        [jax.ShapeDtypeStruct((64, W), BF16), small(WQ), small(WV), small(WQ), small(WV)],
        (message, m_1, m_2, m_3, w16, w_1, w_2, w_3, mq, mv, vq, vv),
        [pltpu.VMEM((64, W), F32)],
    )
    u_1, u_2, u_3 = to_all("major", (u_own,) * 3)
    g_2 = shifted(g_3, "major", 3)
    g_1 = shifted(group, "major", 1)
    u, squares = whole_call(
        assemble_kernel,
        [jax.ShapeDtypeStruct((RANK, W), BF16), jax.ShapeDtypeStruct((8, 128), F32)],
        (u_own, u_1, u_2, u_3),
    )
    s_1, s_2, s_3 = to_all("x", (squares,) * 3)
    chips = (squares + s_2) + (s_1 + s_3)
    other = shifted(chips, "core", 1)
    kept = (first_q, first_v, second_q, second_v)
    new_q, new_v, step_q, step_v, copy_q, copy_v, *kept = new_weights(
        chips, other, u, pq, pv, (group, g_1, g_2, g_3), wq, wv, kept
    )
    return (new_q, new_v, copy_q, copy_v, *kept, step_q, step_v)


def solution(mesh):
    finer = Mesh(mesh.devices.reshape(SIZES), AXES)
    both, tokens, columns = P(FS, TP), P(FS, None), P(None, TP)
    return jax.shard_map(
        on_device,
        mesh=finer,
        in_specs=(tokens, both, both, P(), P()) + (both,) * 6,
        out_specs=(both, both, columns, columns) + (both,) * 6,
        check_vma=False,
    )
```
